1024 devices in a mesh: sp: 128 (over z, y), tp: 8 (over x, core).
Axes of the slice: x: 4, y: 8, z: 16, core: 2. Of those that a mesh axis runs over, the one named last changes fastest.
Arguments:
- tokens: bfloat16 [98304, 2048], P('sp', 'tp'), may hold values from -18 to 18
- proj_weight: bfloat16 [2048, 1024], P(None, 'tp'), may hold values from -0.125 to 0.125
- gate_weight: bfloat16 [2048, 1024], P(None, 'tp'), may hold values from -0.125 to 0.125
- conv_weight: float32 [4, 1024], replicated, may hold values from -3 to 3
- recur_weight: bfloat16 [16, 64, 64], replicated, may hold values from -0.75 to 0.75
- input_weight: bfloat16 [16, 64, 64], replicated, may hold values from -0.75 to 0.75
- decay_param: float32 [1024], replicated, as said below
- out_grad: bfloat16 [98304, 1024], P('sp', 'tp'), may hold values from -6 to 6
Outputs:
- d_proj: bfloat16 [98304, 1024], P('sp', 'tp')
- d_gate: bfloat16 [98304, 1024], P('sp', 'tp')
- d_weight: float32 [2048, 1024], P('sp', 'tp')
The draws below stay inside these ranges and needn't reach their ends.
Inputs may be any that keep to these rules, and one draw needn't show every extreme that they name: `decay_param`: every channel's decay parameter is at least 4; there is no fixed upper bound.
All inputs are finite; a program needn't handle non-finite values.
Results may differ from the reference program's by a relative error of at most 0.01.
Values may be sent and summed in bfloat16 or wider, within the bound.
A program may use at most 32 MiB of HBM per device.

```python
import jax
import jax.numpy as jnp
from jax import lax

D = 2048
CHANNELS = 1024
BLOCK = 64
TOK_DEV = 768
TOKENS = 98304


def draw_tokens(key, part):
    key_base = jax.random.fold_in(key, 11)
    key_scale = jax.random.fold_in(key, 12)
    base = jnp.clip(jax.random.normal(key_base, (TOKENS, D), jnp.float32), -6.0, 6.0)
    span_count = TOKENS // TOK_DEV
    scales = jnp.exp(jax.random.uniform(key_scale, (span_count, 1, 1), jnp.float32, jnp.log(0.4), jnp.log(2.5)))
    shaped = base.reshape(span_count, TOK_DEV, D) * scales
    return shaped.reshape(TOKENS, D).astype(jnp.bfloat16)


def draw_decay_param(key, part):
    key_pick = jax.random.fold_in(key, 21)
    key_slow = jax.random.fold_in(key, 22)
    key_fast = jax.random.fold_in(key, 23)
    slow_pick = jax.random.randint(key_pick, (CHANNELS,), 0, 2) > 0
    slow_value = jnp.log(jnp.float32(TOKENS)) + jax.random.uniform(key_slow, (CHANNELS,), jnp.float32, 0.7, 2.2)
    fast_value = jax.random.uniform(key_fast, (CHANNELS,), jnp.float32, 4.4, 5.3)
    return jnp.where(slow_pick, slow_value, fast_value).astype(jnp.float32)


def block_levels(rng, dims, shards, smallest, largest):
    gain, own = 1.0, jax.random.fold_in(rng, 6)
    for axis_at, blocks in shards:
        steps = jnp.exp(jax.random.uniform(jax.random.fold_in(own, axis_at), (blocks,), jnp.float32, smallest / len(shards), largest / len(shards)))
        gain = gain * jnp.repeat(steps, dims[axis_at] // blocks).reshape([-1 if axis == axis_at else 1 for axis in range(len(dims))])
    return gain


def gaussian(own_key, dims, deviation, reach, shards=(), kind=jnp.bfloat16):
    gain = block_levels(own_key, dims, shards, -0.22, 0.18) if shards else 1.0
    entries = jax.random.normal(own_key, dims, jnp.float32) * deviation * gain
    return jnp.minimum(jnp.maximum(entries, -reach), reach).astype(kind)


def setup_inputs(seed: int = 0) -> dict:
    key_list = jax.random.split(jax.random.key(seed), 9)
    tokens = draw_tokens(jax.random.fold_in(key_list[8], 71), 0)
    proj_weight = gaussian(key_list[1], (D, CHANNELS), D ** -0.5, 0.125, ((1, 8),))
    gate_weight = gaussian(key_list[2], (D, CHANNELS), D ** -0.5, 0.125, ((1, 8),))
    conv_weight = gaussian(key_list[3], (4, CHANNELS), 4 ** -0.5, 3.0, (), jnp.float32)
    recur_weight = gaussian(key_list[4], (CHANNELS // BLOCK, BLOCK, BLOCK), BLOCK ** -0.5, 0.75)
    input_weight = gaussian(key_list[5], (CHANNELS // BLOCK, BLOCK, BLOCK), BLOCK ** -0.5, 0.75)
    decay_param = draw_decay_param(jax.random.fold_in(key_list[8], 71), 0)
    out_grad = gaussian(key_list[7], (TOKENS, CHANNELS), 1.0, 6.0, ((0, 128), (1, 8)))
    return dict(tokens=tokens, proj_weight=proj_weight, gate_weight=gate_weight, conv_weight=conv_weight, recur_weight=recur_weight, input_weight=input_weight, decay_param=decay_param, out_grad=out_grad)


rate_scale = 8.0
scale_floor = 0.0001

def combine(earlier, later):
    return (earlier[0] * later[0], later[0] * earlier[1] + later[1])

def reference(tokens, proj_weight, gate_weight, conv_weight, recur_weight, input_weight, decay_param, out_grad):
    seq_rows = tokens.shape[0]
    group_count = proj_weight.shape[1] // BLOCK

    def per_block(group):
        cols = (group * BLOCK).astype(jnp.int32)
        w_proj = lax.dynamic_slice_in_dim(proj_weight, cols, BLOCK, 1)
        w_gate = lax.dynamic_slice_in_dim(gate_weight, cols, BLOCK, 1)
        conv_taps = lax.dynamic_slice_in_dim(conv_weight, cols, BLOCK, 1)
        decay_slice = lax.dynamic_slice_in_dim(decay_param, cols, BLOCK, 0)
        w_recur = lax.dynamic_index_in_dim(recur_weight, group.astype(jnp.int32), 0, False)
        w_input = lax.dynamic_index_in_dim(input_weight, group.astype(jnp.int32), 0, False)
        cotangent = lax.dynamic_slice_in_dim(out_grad, cols, BLOCK, 1).astype(jnp.float32)
        projected = jnp.dot(tokens, w_proj, preferred_element_type=jnp.float32).astype(jnp.bfloat16)
        gate_in = jnp.dot(tokens, w_gate, preferred_element_type=jnp.float32).astype(jnp.bfloat16)
        padded = jnp.concatenate([jnp.zeros((3, BLOCK), jnp.float32), projected.astype(jnp.float32)], axis=0)
        total = conv_taps[0] * padded[3:3 + seq_rows]
        for offset in range(1, 4):
            total = total + conv_taps[offset] * padded[3 - offset:3 - offset + seq_rows]
        conv_out = total.astype(jnp.bfloat16)
        conv_float = conv_out.astype(jnp.float32)
        recur_pre = jnp.dot(conv_out, w_recur, preferred_element_type=jnp.float32)
        input_pre = jnp.dot(conv_out, w_input, preferred_element_type=jnp.float32)
        recur_open = jax.nn.sigmoid(recur_pre)
        input_open = jax.nn.sigmoid(input_pre)
        log_slope = rate_scale * jax.nn.log_sigmoid(decay_slice)
        log_decay = log_slope * recur_open
        decay_rate = jnp.exp(log_decay)
        input_scale = jnp.sqrt(scale_floor - jnp.expm1(2.0 * log_decay))
        gated_input = input_open * conv_float
        drive = input_scale * gated_input
        _, states = lax.associative_scan(combine, (decay_rate, drive), axis=0)
        previous = jnp.concatenate([jnp.zeros((1, BLOCK), jnp.float32), states[:-1]], axis=0)
        gelu_gate, gelu_back = jax.vjp(jax.nn.gelu, gate_in.astype(jnp.float32))
        d_gate = gelu_back(cotangent * states)[0].astype(jnp.bfloat16)
        drive_grad = cotangent * gelu_gate
        shifted = jnp.concatenate([decay_rate[1:], jnp.ones((1, BLOCK), jnp.float32)], axis=0)
        _, state_grad = lax.associative_scan(combine, (shifted, drive_grad), reverse=True, axis=0)
        d_log_decay = state_grad * (decay_rate * previous - gated_input * decay_rate * decay_rate / input_scale)
        d_recur_pre = (d_log_decay * log_slope * recur_open * (1.0 - recur_open)).astype(jnp.bfloat16)
        d_input_pre = (state_grad * input_scale * conv_float * input_open * (1.0 - input_open)).astype(jnp.bfloat16)
        d_conv = state_grad * input_scale * input_open
        d_conv = d_conv + jnp.dot(d_recur_pre, w_recur.T, preferred_element_type=jnp.float32)
        d_conv = d_conv + jnp.dot(d_input_pre, w_input.T, preferred_element_type=jnp.float32)
        extended = jnp.concatenate([d_conv, jnp.zeros((3, BLOCK), jnp.float32)], axis=0)
        grad_sum = conv_taps[0] * extended[0:seq_rows]
        for offset in range(1, 4):
            grad_sum = grad_sum + conv_taps[offset] * extended[offset:offset + seq_rows]
        d_proj = grad_sum.astype(jnp.bfloat16)
        d_weight = lax.dot_general(tokens, d_proj, (((0,), (0,)), ((), ())), preferred_element_type=jnp.float32)
        return (d_proj, d_gate, d_weight)
    d_proj, d_gate, d_weight = lax.map(per_block, jnp.arange(group_count, dtype=jnp.int32))
    d_proj = jnp.transpose(d_proj, (1, 0, 2)).reshape(seq_rows, group_count * BLOCK)
    d_gate = jnp.transpose(d_gate, (1, 0, 2)).reshape(seq_rows, group_count * BLOCK)
    d_weight = jnp.transpose(d_weight, (1, 0, 2)).reshape(d_weight.shape[1], group_count * BLOCK)
    return (d_proj, d_gate, d_weight)
```

```python
import functools

import jax
import jax.numpy as jnp
from jax import lax
from jax.experimental import pallas as pl
from jax.experimental.pallas import tpu as pltpu
from jax.sharding import Mesh
from jax.sharding import PartitionSpec as P

MESH = pl.DeviceIdType.MESH
F32 = jnp.float32
BF16 = jnp.bfloat16
BLOCK = 64
HALO = 16
LANES = 128
RATE = 8.0
FLOOR = 0.0001
GELU_A = 0.7978845608028654
GELU_B = 0.044715
CHUNK = 80


def small_expm1(x):
    p = 1.0 / 5040.0
    for c in (1.0 / 720.0, 1.0 / 120.0, 1.0 / 24.0, 1.0 / 6.0, 0.5, 1.0):
        p = p * x + c
    return p * x


def small_log1p(u):
    p = -1.0 / 6.0
    for c in (1.0 / 5.0, -1.0 / 4.0, 1.0 / 3.0, -0.5, 1.0):
        p = p * u + c
    return p * u


def kernel(
    dims, tok, pw, gw, cw, rw, iw, dp, og, dproj, dgate, dweight,
    G, WP, WG, OG, RW, IW, ACC, PJ, CV, PRE, A, B, DG, RO, IO, SC, DGL, HP, PP, YN, QN, DR, DC,
    SUM, RYC, SUMZ, RZC, CF, CB, WS, RY, VZ, RZ,
    lsem, hps, hpr, hns, hnr, ogs, ags, agr, ycs, ycr, zcs, zcr, rys, ryr, rzs, rzr,
):
    NZ, NY, NX, rows = dims
    R = rows + 2 * HALO
    SEG = R // 8
    nch = R // CHUNK
    z, y, x, c = (lax.axis_index(n) for n in ("z", "y", "x", "c"))
    sp = z * NY + y
    nsp = NZ * NY
    tp = x * 2 + c
    nxt, prv = lax.rem(sp + 1, nsp), lax.rem(sp + nsp - 1, nsp)
    nz, ny = nxt // NY, lax.rem(nxt, NY)
    pz, py = prv // NY, lax.rem(prv, NY)
    left, right, opp = lax.rem(x + NX - 1, NX), lax.rem(x + 1, NX), lax.rem(x + 2, NX)

    loads = [
        pltpu.make_async_copy(tok.at[:, pl.ds(h * LANES, LANES)], G.at[2 * tp + h, pl.ds(HALO, rows)], lsem.at[h])
        for h in range(2)
    ]
    loads += [
        pltpu.make_async_copy(pw, WP, lsem.at[2]),
        pltpu.make_async_copy(gw, WG, lsem.at[3]),
        pltpu.make_async_copy(og, OG.at[pl.ds(HALO, rows)], lsem.at[4]),
        pltpu.make_async_copy(rw.at[pl.ds(2 * tp, 2)], RW, lsem.at[5]),
        pltpu.make_async_copy(iw.at[pl.ds(2 * tp, 2)], IW, lsem.at[6]),
    ]
    for copy in loads:
        copy.start()

    barrier = pltpu.get_barrier_semaphore()

    def greet(**where):
        pl.semaphore_signal(barrier, inc=1, device_id=where, device_id_type=MESH)

    greet(c=1 - c)
    greet(x=left)
    greet(x=right)
    for k in range(NX):
        for d in range(2):
            greet(z=nz, y=ny, x=k, c=d)
            greet(z=pz, y=py, x=k, c=d)
    for d in range(1, NY):
        greet(y=lax.rem(y + d, NY))
    for d in range(1, NZ):
        greet(z=lax.rem(z + d, NZ))
    pl.semaphore_wait(barrier, 3 + 4 * NX + NY - 1 + NZ - 1)

    pending = []

    def send(src, dst, ssem, rsem, **where):
        copy = pltpu.make_async_remote_copy(
            src_ref=src, dst_ref=dst, send_sem=ssem, recv_sem=rsem, device_id=where, device_id_type=MESH
        )
        copy.start()
        pending.append(copy)

    def arrived(dst, ssem, rsem, **where):
        pltpu.make_async_remote_copy(
            src_ref=dst, dst_ref=dst, send_sem=ssem, recv_sem=rsem, device_id=where, device_id_type=MESH
        ).wait_recv()

    loads[0].wait()
    loads[1].wait()
    mine = 2 * tp
    main = pl.ds(HALO, rows)
    for k in range(NX):
        for d in range(2):
            n = 2 * k + d
            send(G.at[pl.ds(mine, 2), pl.ds(rows, HALO)], G.at[pl.ds(mine, 2), pl.ds(0, HALO)],
                 hps.at[n], hpr.at[tp], z=nz, y=ny, x=k, c=d)
            send(G.at[pl.ds(mine, 2), pl.ds(HALO, HALO)], G.at[pl.ds(mine, 2), pl.ds(HALO + rows, HALO)],
                 hns.at[n], hnr.at[tp], z=pz, y=py, x=k, c=d)

    def piece(xx, cc, h):
        return 4 * xx + 2 * cc + h

    def give(i, sem, **where):
        send(G.at[i, main], G.at[i, main], ags.at[sem], agr.at[sem], **where)

    def got(i, sem):
        arrived(G.at[i, main], ags.at[sem], agr.at[sem], c=1 - c)

    p0, p1 = piece(x, c, 0), piece(x, c, 1)
    give(p0, 0, x=right)
    give(p1, 1, x=left)
    give(p1, 2, x=right)
    give(p0, 3, x=left)
    give(p0, 6, c=1 - c)
    give(p1, 7, c=1 - c)
    loads[4].wait()
    send(OG.at[pl.ds(HALO, HALO)], OG.at[pl.ds(HALO + rows, HALO)], ogs.at[0], ogs.at[1], z=pz, y=py)
    for k in (2, 3, 5, 6):
        loads[k].wait()

    OG[pl.ds(0, HALO), :] = jnp.zeros((HALO, LANES), BF16)
    PJ[pl.ds(0, 8), :] = jnp.zeros((8, LANES), F32)
    DC[pl.ds(R, 8), :] = jnp.zeros((8, LANES), F32)
    slope = -RATE * small_log1p(jnp.exp(-dp[pl.ds(tp, 1), :]))
    taps = [cw[pl.ds(k, 1), pl.ds(pl.multiple_of(tp * LANES, LANES), LANES)] for k in range(4)]
    zero = jnp.zeros((BLOCK, BLOCK), BF16)
    gates = jnp.concatenate(
        [
            jnp.concatenate([RW[0], zero, IW[0], zero], axis=1),
            jnp.concatenate([zero, RW[1], zero, IW[1]], axis=1),
        ],
        axis=0,
    )

    for n in range(2 * NX):
        arrived(G.at[pl.ds(2 * n, 2), pl.ds(0, HALO)], hps.at[n], hpr.at[n], c=1 - c)
        arrived(G.at[pl.ds(2 * n, 2), pl.ds(HALO + rows, HALO)], hns.at[n], hnr.at[n], c=1 - c)
    arrived(OG.at[pl.ds(HALO + rows, HALO)], ogs.at[0], ogs.at[1], c=1 - c)

    @pl.when(sp == 0)
    def _():
        G[:, pl.ds(0, HALO), :] = jnp.zeros((4 * NX, HALO, LANES), BF16)

    @pl.when(sp == nsp - 1)
    def _():
        G[:, pl.ds(HALO + rows, HALO), :] = jnp.zeros((4 * NX, HALO, LANES), BF16)
        OG[pl.ds(HALO + rows, HALO), :] = jnp.zeros((HALO, LANES), BF16)

    def multiply(i0, i1, first=False):
        def half(i):
            at = pl.ds(pl.multiple_of(i * LANES, LANES), LANES)
            return jnp.concatenate([WP[at, :], WG[at, :]], axis=1)

        rhs = jnp.concatenate([half(i0), half(i1)], axis=0)
        lhs = jnp.concatenate([G[i0], G[i1]], axis=1)
        out = jnp.dot(lhs, rhs, preferred_element_type=F32)
        if first:
            ACC[...] = out
        else:
            ACC[...] += out

    multiply(p0, p1, True)
    got(piece(x, 1 - c, 0), 6)
    got(piece(x, 1 - c, 1), 7)
    multiply(piece(x, 1 - c, 0), piece(x, 1 - c, 1))

    l0, l1 = piece(left, c, 0), piece(left, c, 1)
    r0, r1 = piece(right, c, 0), piece(right, c, 1)
    o0, o1 = piece(opp, c, 0), piece(opp, c, 1)
    got(l0, 0)
    give(l0, 4, x=right)
    give(l0, 8, c=1 - c)
    got(r1, 1)
    give(r1, 5, x=left)
    give(r1, 9, c=1 - c)
    multiply(l0, r1)
    got(piece(left, 1 - c, 0), 8)
    got(piece(right, 1 - c, 1), 9)
    multiply(piece(left, 1 - c, 0), piece(right, 1 - c, 1))
    got(l1, 2)
    give(l1, 10, c=1 - c)
    got(r0, 3)
    give(r0, 11, c=1 - c)
    multiply(l1, r0)
    got(piece(left, 1 - c, 1), 10)
    got(piece(right, 1 - c, 0), 11)
    multiply(piece(left, 1 - c, 1), piece(right, 1 - c, 0))
    got(o0, 4)
    give(o0, 12, c=1 - c)
    got(o1, 5)
    give(o1, 13, c=1 - c)
    multiply(o0, o1)
    got(piece(opp, 1 - c, 0), 12)
    got(piece(opp, 1 - c, 1), 13)
    multiply(piece(opp, 1 - c, 0), piece(opp, 1 - c, 1))

    PJ[pl.ds(8, R), :] = ACC[:, pl.ds(0, LANES)].astype(BF16).astype(F32)

    def convolve(i, _):
        base = pl.multiple_of(i * CHUNK, CHUNK)
        part = PJ[pl.ds(base, CHUNK + 8), :]
        total = taps[0] * part[8:]
        for k in range(1, 4):
            total = total + taps[k] * pltpu.roll(part, k, 0)[8:]
        CV[pl.ds(base, CHUNK), :] = total.astype(BF16)
        return 0

    lax.fori_loop(0, nch, convolve, 0)
    PRE[...] = jnp.dot(CV[...], gates, preferred_element_type=F32)

    def local(i, _):
        base = pl.multiple_of(i * CHUNK, CHUNK)
        at = pl.ds(base, CHUNK)
        ro = jax.nn.sigmoid(PRE[at, pl.ds(0, LANES)])
        io = jax.nn.sigmoid(PRE[at, pl.ds(LANES, LANES)])
        conv = CV[at, :].astype(F32)
        e = small_expm1(slope * ro)
        sc = jnp.sqrt(FLOOR - e * (2.0 + e))
        row = lax.broadcasted_iota(jnp.int32, (CHUNK, LANES), 0) + base
        own = row >= HALO
        A[at, :] = jnp.where(own, 1.0 + e, 1.0)
        B[at, :] = jnp.where(own, sc * (io * conv), 0.0)
        RO[at, :] = ro
        IO[at, :] = io
        SC[at, :] = sc
        q = ACC[at, pl.ds(LANES, LANES)].astype(BF16).astype(F32)
        cot = OG[at, :].astype(F32)
        t = jnp.tanh(GELU_A * (q + GELU_B * (q * q * q)))
        cdf = 0.5 * (1.0 + t)
        DG[at, :] = cot * (q * cdf)
        DGL[at, :] = cot * (cdf + 0.5 * q * (1.0 - t * t) * (GELU_A * (1.0 + 3.0 * GELU_B * (q * q))))
        return 0

    lax.fori_loop(0, nch, local, 0)

    STEP = 10

    def scan(i, carry):
        h, p, yb, q = carry
        for k in range(STEP):
            v = i * STEP + k
            fw, bw = pl.ds(v, 8, stride=SEG), pl.ds(SEG - 1 - v, 8, stride=SEG)
            a, b = A[fw, :], B[fw, :]
            HP[fw, :] = h
            PP[fw, :] = p
            h = a * h + b
            p = p * a
            a, g = A[bw, :], DG[bw, :]
            YN[bw, :] = yb
            QN[bw, :] = q
            yb = a * (g + yb)
            q = q * a
        return h, p, yb, q

    one, nil = jnp.ones((8, LANES), F32), jnp.zeros((8, LANES), F32)
    h, p, yb, q = lax.fori_loop(0, SEG // STEP, scan, (nil, one, nil, one))

    fa, fs, s_of, a_of = one[0:1], nil[0:1], [], []
    for k in range(8):
        s_of.append(fs)
        a_of.append(fa)
        fs = h[k : k + 1] + p[k : k + 1] * fs
        fa = fa * p[k : k + 1]
    ba, bs, t_of, c_of = one[0:1], nil[0:1], [None] * 8, [None] * 8
    for k in reversed(range(8)):
        t_of[k] = bs
        c_of[k] = ba
        bs = yb[k : k + 1] + q[k : k + 1] * bs
        ba = ba * q[k : k + 1]
    last, lead = HALO + rows - 1, 2 * HALO
    ls, fsg = last // SEG, lead // SEG
    la, lb = A[pl.ds(last, 1), :], B[pl.ds(last, 1), :]
    lp = PP[pl.ds(last, 1), :]
    out_a = la * lp * a_of[ls]
    out_s = la * (HP[pl.ds(last, 1), :] + lp * s_of[ls]) + lb
    ga, gg = A[pl.ds(lead, 1), :], DG[pl.ds(lead, 1), :]
    gq = QN[pl.ds(lead, 1), :]
    out_c = ga * gq * c_of[fsg]
    out_l = ga * (gg + YN[pl.ds(lead, 1), :] + gq * t_of[fsg])

    def put(ref, values):
        for k, value in enumerate(values):
            ref[pl.ds(k, 1), :] = value

    SUM[...] = nil
    put(SUM, (out_a, out_s, out_c, out_l))
    for d in range(1, NY):
        send(SUM, RYC.at[y], ycs.at[d], ycr.at[y], y=lax.rem(y + d, NY))
    RYC[y] = SUM[...]
    for d in range(1, NY):
        k = lax.rem(y + d, NY)
        arrived(RYC.at[k], ycs.at[d], ycr.at[k], c=1 - c)

    def compose(ref, count, place):
        fa, fs, fai, fsi = one[0:1], nil[0:1], one[0:1], nil[0:1]
        for k in range(count):
            a, s = ref[k, pl.ds(0, 1), :], ref[k, pl.ds(1, 1), :]
            fa, fs = fa * a, a * fs + s
            before = k < place
            fai, fsi = jnp.where(before, fa, fai), jnp.where(before, fs, fsi)
        ba, bs, bai, bsi = one[0:1], nil[0:1], one[0:1], nil[0:1]
        for k in reversed(range(count)):
            a, s = ref[k, pl.ds(2, 1), :], ref[k, pl.ds(3, 1), :]
            ba, bs = ba * a, a * bs + s
            after = k > place
            bai, bsi = jnp.where(after, ba, bai), jnp.where(after, bs, bsi)
        return (fa, fs, ba, bs), (fai, fsi, bai, bsi)

    total, inside = compose(RYC, NY, y)
    SUMZ[...] = nil
    put(SUMZ, total)
    for d in range(1, NZ):
        send(SUMZ, RZC.at[z], zcs.at[d], zcr.at[z], z=lax.rem(z + d, NZ))
    RZC[z] = SUMZ[...]
    for d in range(1, NZ):
        k = lax.rem(z + d, NZ)
        arrived(RZC.at[k], zcs.at[d], zcr.at[k], c=1 - c)
    _, outer = compose(RZC, NZ, z)
    carry_s = inside[1] + inside[0] * outer[1]
    carry_g = inside[3] + inside[2] * outer[3]
    put(CF, [s_of[k] + a_of[k] * carry_s for k in range(8)])
    put(CB, [t_of[k] + c_of[k] * carry_g for k in range(8)])
    cf, cb = CF[...], CB[...]

    def finish(i, _):
        for k in range(STEP):
            at = pl.ds(i * STEP + k, 8, stride=SEG)
            HP[at, :] = HP[at, :] + PP[at, :] * cf
            YN[at, :] = YN[at, :] + QN[at, :] * cb
        return 0

    lax.fori_loop(0, SEG // STEP, finish, 0)

    def gradients(i, _):
        base = pl.multiple_of(i * CHUNK, CHUNK)
        at = pl.ds(base, CHUNK)
        a, ro, io, sc = A[at, :], RO[at, :], IO[at, :], SC[at, :]
        conv = CV[at, :].astype(F32)
        decayed = a * HP[at, :]
        grad = DG[at, :] + YN[at, :]
        gated = io * conv
        DGL[at, :] = DGL[at, :] * (decayed + B[at, :])
        d_log = grad * (decayed - gated * a * a / sc)
        DR[at, pl.ds(0, LANES)] = (d_log * slope * ro * (1.0 - ro)).astype(BF16)
        gs = grad * sc
        DR[at, pl.ds(LANES, LANES)] = (gs * conv * io * (1.0 - io)).astype(BF16)
        DC[at, :] = gs * io
        return 0

    lax.fori_loop(0, nch, gradients, 0)
    dgate[...] = DGL[pl.ds(HALO, rows), :].astype(BF16)
    DC[pl.ds(0, R), :] += lax.dot_general(DR[...], gates, (((1,), (1,)), ((), ())), preferred_element_type=F32)

    WIDE = 96

    def unconvolve(i, _):
        base = pl.multiple_of(i * WIDE, WIDE)
        part = DC[pl.ds(base + HALO, WIDE + 8), :]
        total = taps[0] * part[:WIDE]
        for k in range(1, 4):
            total = total + taps[k] * pltpu.roll(part, WIDE + 8 - k, 0)[:WIDE]
        dproj[pl.ds(base, WIDE), :] = total.astype(BF16)
        return 0

    lax.fori_loop(0, rows // WIDE, unconvolve, 0)

    grad = dproj[...]
    share = LANES // NY
    per = NZ // 4
    for g in range(4):
        for i in range(g * per, (g + 1) * per):
            part = lax.dot_general(G[i, main, :], grad, (((0,), (0,)), ((), ())), preferred_element_type=F32)
            WS[:, i] = part.astype(BF16).reshape(NY, share, LANES)
        for d in range(1, NY):
            k = lax.rem(y + d, NY)
            send(WS.at[k, pl.ds(g * per, per)], RY.at[y, pl.ds(g * per, per)], rys.at[g, d], ryr.at[g, y], y=k)
    for g in range(4):
        total = WS[y, pl.ds(g * per, per)].astype(F32)
        for d in range(1, NY):
            k = lax.rem(y + d, NY)
            arrived(RY.at[k, pl.ds(g * per, per)], rys.at[g, d], ryr.at[g, k], c=1 - c)
            total = total + RY[k, pl.ds(g * per, per)].astype(F32)
        VZ[pl.ds(g * per, per)] = total.astype(BF16)
    for d in range(1, NZ):
        k = lax.rem(z + d, NZ)
        send(VZ.at[k], RZ.at[z], rzs.at[d], rzr.at[z], z=k)
    total = VZ[z].astype(F32)
    for d in range(1, NZ):
        k = lax.rem(z + d, NZ)
        arrived(RZ.at[k], rzs.at[d], rzr.at[k], c=1 - c)
        total = total + RZ[k].astype(F32)
    dweight[...] = total
    for copy in pending:
        copy.wait_send()


def per_device(dims, tokens, proj_weight, gate_weight, conv_weight, recur_weight, input_weight, decay_param, out_grad):
    NZ, NY, NX, rows = dims
    R = rows + 2 * HALO
    share = LANES // NY
    vmem = pltpu.VMEM
    dma = pltpu.SemaphoreType.DMA
    flat = [vmem((R, LANES), F32)] * 11
    anywhere, inside = pl.BlockSpec(memory_space=pl.ANY), pl.BlockSpec(memory_space=pltpu.VMEM)
    return pl.pallas_call(
        functools.partial(kernel, dims),
        out_shape=(
            jax.ShapeDtypeStruct((rows, LANES), BF16),
            jax.ShapeDtypeStruct((rows, LANES), BF16),
            jax.ShapeDtypeStruct((share, LANES), F32),
        ),
        in_specs=[anywhere, anywhere, anywhere, inside, anywhere, anywhere, inside, anywhere],
        out_specs=(inside, inside, inside),
        scratch_shapes=[
            vmem((4 * NX, R, LANES), BF16),
            vmem(proj_weight.shape, BF16),
            vmem(gate_weight.shape, BF16),
            vmem((R, LANES), BF16),
            vmem((2, BLOCK, BLOCK), BF16),
            vmem((2, BLOCK, BLOCK), BF16),
            vmem((R, 2 * LANES), F32),
            vmem((R + 8, LANES), F32),
            vmem((R, LANES), BF16),
            vmem((R, 2 * LANES), F32),
            *flat,
            vmem((R, 2 * LANES), BF16),
            vmem((R + 8, LANES), F32),
            vmem((8, LANES), F32),
            vmem((NY, 8, LANES), F32),
            vmem((8, LANES), F32),
            vmem((NZ, 8, LANES), F32),
            vmem((8, LANES), F32),
            vmem((8, LANES), F32),
            vmem((NY, NZ, share, LANES), BF16),
            vmem((NY, NZ, share, LANES), BF16),
            vmem((NZ, share, LANES), BF16),
            vmem((NZ, share, LANES), BF16),
            dma((7,)),
            dma((2 * NX,)),
            dma((2 * NX,)),
            dma((2 * NX,)),
            dma((2 * NX,)),
            dma((2,)),
            dma((14,)),
            dma((14,)),
            dma((NY,)),
            dma((NY,)),
            dma((NZ,)),
            dma((NZ,)),
            dma((4, NY)),
            dma((4, NY)),
            dma((NZ,)),
            dma((NZ,)),
        ],
        compiler_params=pltpu.CompilerParams(collective_id=0, has_side_effects=True),
    )(
        tokens, proj_weight, gate_weight, conv_weight, recur_weight, input_weight,
        decay_param.reshape(-1, LANES), out_grad,
    )


def solution(mesh):
    sizes = (16, 8, 4, 2)
    split = Mesh(mesh.devices.reshape(sizes), ("z", "y", "x", "c"))
    span, group = ("z", "y"), ("x", "c")
    placed = (P(span, group), P(None, group), P(None, group), P(), P(), P(), P(), P(span, group))

    def step(*args):
        return per_device((*sizes[:3], args[0].shape[0]), *args)

    return jax.shard_map(
        step,
        mesh=split,
        in_specs=placed,
        out_specs=(P(span, group), P(span, group), P(span, group)),
        check_vma=False,
    )
```

```python
import functools

import jax
import jax.numpy as jnp
from jax import lax
from jax.experimental import pallas as pl
from jax.experimental.pallas import tpu as pltpu
from jax.sharding import Mesh
from jax.sharding import PartitionSpec as P

MESH = pl.DeviceIdType.MESH
F32 = jnp.float32
BF16 = jnp.bfloat16
BLOCK = 64
HALO = 16
LANES = 128
RATE = 8.0
FLOOR = 0.0001
GELU_A = 0.7978845608028654
GELU_B = 0.044715
CHUNK = 80


def small_expm1(x):
    p = 1.0 / 5040.0
    for c in (1.0 / 720.0, 1.0 / 120.0, 1.0 / 24.0, 1.0 / 6.0, 0.5, 1.0):
        p = p * x + c
    return p * x


def small_log1p(u):
    p = -1.0 / 6.0
    for c in (1.0 / 5.0, -1.0 / 4.0, 1.0 / 3.0, -0.5, 1.0):
        p = p * u + c
    return p * u


def kernel(
    dims, tok, pw, gw, cw_far, rw, iw, dp_far, og, dproj, dgate, dweight,
    G, WP, WG, OG, RW, IW, ACC, PJ, CV, PRE, A, B, DG, RO, IO, SC, DGL, HP, PP, YN, QN, DR, DC,
    GT, SUM, RYC, SUMZ, RZC, CF, CB, WS, RY, VZ, RZ,
    lsem, hps, hpr, hns, hnr, ogs, ags, agr, ycs, ycr, zcs, zcr, rys, ryr, rzs, rzr, met, cw, dp,
):
    NZ, NY, NX, rows = dims
    R = rows + 2 * HALO
    SEG = R // 8
    nch = R // CHUNK
    z, y, x, c = (lax.axis_index(n) for n in ("z", "y", "x", "c"))
    sp = z * NY + y
    nsp = NZ * NY
    tp = x * 2 + c
    nxt, prv = lax.rem(sp + 1, nsp), lax.rem(sp + nsp - 1, nsp)
    nz, ny = nxt // NY, lax.rem(nxt, NY)
    pz, py = prv // NY, lax.rem(prv, NY)
    left, right, opp = lax.rem(x + NX - 1, NX), lax.rem(x + 1, NX), lax.rem(x + 2, NX)

    loads = [
        pltpu.make_async_copy(tok.at[:, pl.ds(h * LANES, LANES)], G.at[2 * tp + h, pl.ds(HALO, rows)], lsem.at[h])
        for h in range(2)
    ]
    loads += [
        pltpu.make_async_copy(pw, WP, lsem.at[2]),
        pltpu.make_async_copy(gw, WG, lsem.at[3]),
        pltpu.make_async_copy(og, OG.at[pl.ds(HALO, rows)], lsem.at[4]),
        pltpu.make_async_copy(rw.at[pl.ds(2 * tp, 2)], RW, lsem.at[5]),
        pltpu.make_async_copy(iw.at[pl.ds(2 * tp, 2)], IW, lsem.at[6]),
        pltpu.make_async_copy(cw_far, cw, lsem.at[7]),
        pltpu.make_async_copy(dp_far, dp, lsem.at[8]),
    ]
    for copy in loads:
        copy.start()

    barrier = pltpu.get_barrier_semaphore()

    def greet(**where):
        pl.semaphore_signal(barrier, inc=1, device_id=where, device_id_type=MESH)

    greet(c=1 - c)
    greet(x=left)
    greet(x=right)
    for k in range(NX):
        for d in range(2):
            greet(z=nz, y=ny, x=k, c=d)
            greet(z=pz, y=py, x=k, c=d)
    for d in (1, NY - 1):
        greet(y=lax.rem(y + d, NY))
    for d in (1, NZ - 1):
        greet(z=lax.rem(z + d, NZ))
    pl.semaphore_wait(barrier, 3 + 4 * NX + 4)

    def tell(sem, **where):
        pl.semaphore_signal(met.at[sem], inc=1, device_id=where, device_id_type=MESH)

    def tell_y(sem, d):
        tell(sem, y=lax.rem(y + d, NY))
        tell(sem, y=lax.rem(y + NY - d, NY))

    def tell_z(sem, d):
        tell(sem, z=lax.rem(z + d, NZ))
        tell(sem, z=lax.rem(z + NZ - d, NZ))

    far_y = sorted(range(1, NY), key=lambda d: -min(d, NY - d))
    far_z = sorted(range(1, NZ), key=lambda d: -min(d, NZ - d))
    pending = []

    def send(src, dst, ssem, rsem, **where):
        copy = pltpu.make_async_remote_copy(
            src_ref=src, dst_ref=dst, send_sem=ssem, recv_sem=rsem, device_id=where, device_id_type=MESH
        )
        copy.start()
        pending.append(copy)

    def arrived(dst, ssem, rsem, **where):
        pltpu.make_async_remote_copy(
            src_ref=dst, dst_ref=dst, send_sem=ssem, recv_sem=rsem, device_id=where, device_id_type=MESH
        ).wait_recv()

    loads[0].wait()
    loads[1].wait()
    mine = 2 * tp
    main = pl.ds(HALO, rows)
    for k in range(NX):
        for d in range(2):
            n = 2 * k + d
            send(G.at[pl.ds(mine, 2), pl.ds(rows, HALO)], G.at[pl.ds(mine, 2), pl.ds(0, HALO)],
                 hps.at[n], hpr.at[tp], z=nz, y=ny, x=k, c=d)
            send(G.at[pl.ds(mine, 2), pl.ds(HALO, HALO)], G.at[pl.ds(mine, 2), pl.ds(HALO + rows, HALO)],
                 hns.at[n], hnr.at[tp], z=pz, y=py, x=k, c=d)

    def piece(xx, cc, h):
        return 4 * xx + 2 * cc + h

    def give(i, sem, **where):
        send(G.at[i, main], G.at[i, main], ags.at[sem], agr.at[sem], **where)

    def got(i, sem):
        arrived(G.at[i, main], ags.at[sem], agr.at[sem], c=1 - c)

    p0, p1 = piece(x, c, 0), piece(x, c, 1)
    give(p0, 0, x=right)
    give(p1, 1, x=left)
    give(p1, 2, x=right)
    give(p0, 3, x=left)
    give(p0, 6, c=1 - c)
    give(p1, 7, c=1 - c)
    loads[4].wait()
    send(OG.at[pl.ds(HALO, HALO)], OG.at[pl.ds(HALO + rows, HALO)], ogs.at[0], ogs.at[1], z=pz, y=py)
    tell_y(0, 1)
    tell_z(1, 1)
    for k in (2, 3, 5, 6, 7, 8):
        loads[k].wait()

    OG[pl.ds(0, HALO), :] = jnp.zeros((HALO, LANES), BF16)
    PJ[pl.ds(0, 8), :] = jnp.zeros((8, LANES), F32)
    DC[pl.ds(R, 8), :] = jnp.zeros((8, LANES), F32)
    slope = -RATE * small_log1p(jnp.exp(-dp[pl.ds(tp, 1), :]))
    taps = [cw[pl.ds(k, 1), pl.ds(pl.multiple_of(tp * LANES, LANES), LANES)] for k in range(4)]
    zero = jnp.zeros((BLOCK, BLOCK), BF16)
    gates = jnp.concatenate(
        [
            jnp.concatenate([RW[0], zero, IW[0], zero], axis=1),
            jnp.concatenate([zero, RW[1], zero, IW[1]], axis=1),
        ],
        axis=0,
    )

    for n in range(2 * NX):
        arrived(G.at[pl.ds(2 * n, 2), pl.ds(0, HALO)], hps.at[n], hpr.at[n], c=1 - c)
        arrived(G.at[pl.ds(2 * n, 2), pl.ds(HALO + rows, HALO)], hns.at[n], hnr.at[n], c=1 - c)
    arrived(OG.at[pl.ds(HALO + rows, HALO)], ogs.at[0], ogs.at[1], c=1 - c)

    @pl.when(sp == 0)
    def _():
        G[:, pl.ds(0, HALO), :] = jnp.zeros((4 * NX, HALO, LANES), BF16)

    @pl.when(sp == nsp - 1)
    def _():
        G[:, pl.ds(HALO + rows, HALO), :] = jnp.zeros((4 * NX, HALO, LANES), BF16)
        OG[pl.ds(HALO + rows, HALO), :] = jnp.zeros((HALO, LANES), BF16)

    def multiply(i0, i1, first=False):
        def half(i):
            at = pl.ds(pl.multiple_of(i * LANES, LANES), LANES)
            return jnp.concatenate([WP[at, :], WG[at, :]], axis=1)

        rhs = jnp.concatenate([half(i0), half(i1)], axis=0)
        lhs = jnp.concatenate([G[i0], G[i1]], axis=1)
        out = jnp.dot(lhs, rhs, preferred_element_type=F32)
        if first:
            ACC[...] = out
        else:
            ACC[...] += out

    pl.semaphore_wait(met.at[0], 2)
    pl.semaphore_wait(met.at[1], 2)
    tell_y(2, 2)
    tell_z(3, 2)
    multiply(p0, p1, True)
    got(piece(x, 1 - c, 0), 6)
    got(piece(x, 1 - c, 1), 7)
    multiply(piece(x, 1 - c, 0), piece(x, 1 - c, 1))

    l0, l1 = piece(left, c, 0), piece(left, c, 1)
    r0, r1 = piece(right, c, 0), piece(right, c, 1)
    o0, o1 = piece(opp, c, 0), piece(opp, c, 1)
    got(l0, 0)
    give(l0, 4, x=right)
    give(l0, 8, c=1 - c)
    got(r1, 1)
    give(r1, 5, x=left)
    give(r1, 9, c=1 - c)
    multiply(l0, r1)
    got(piece(left, 1 - c, 0), 8)
    got(piece(right, 1 - c, 1), 9)
    multiply(piece(left, 1 - c, 0), piece(right, 1 - c, 1))
    pl.semaphore_wait(met.at[2], 2)
    pl.semaphore_wait(met.at[3], 2)
    tell_z(4, 4)
    got(l1, 2)
    give(l1, 10, c=1 - c)
    got(r0, 3)
    give(r0, 11, c=1 - c)
    multiply(l1, r0)
    got(piece(left, 1 - c, 1), 10)
    got(piece(right, 1 - c, 0), 11)
    multiply(piece(left, 1 - c, 1), piece(right, 1 - c, 0))
    pl.semaphore_wait(met.at[4], 2)
    got(o0, 4)
    give(o0, 12, c=1 - c)
    got(o1, 5)
    give(o1, 13, c=1 - c)
    multiply(o0, o1)
    got(piece(opp, 1 - c, 0), 12)
    got(piece(opp, 1 - c, 1), 13)
    multiply(piece(opp, 1 - c, 0), piece(opp, 1 - c, 1))

    PJ[pl.ds(8, R), :] = ACC[:, pl.ds(0, LANES)].astype(BF16).astype(F32)

    def convolve(i, _):
        base = pl.multiple_of(i * CHUNK, CHUNK)
        part = PJ[pl.ds(base, CHUNK + 8), :]
        total = taps[0] * part[8:]
        for k in range(1, 4):
            total = total + taps[k] * pltpu.roll(part, k, 0)[8:]
        CV[pl.ds(base, CHUNK), :] = total.astype(BF16)
        return 0

    lax.fori_loop(0, nch, convolve, 0)
    PRE[...] = jnp.dot(CV[...], gates, preferred_element_type=F32)

    def local(i, _):
        base = pl.multiple_of(i * CHUNK, CHUNK)
        at = pl.ds(base, CHUNK)
        ro = jax.nn.sigmoid(PRE[at, pl.ds(0, LANES)])
        io = jax.nn.sigmoid(PRE[at, pl.ds(LANES, LANES)])
        conv = CV[at, :].astype(F32)
        e = small_expm1(slope * ro)
        sc = jnp.sqrt(FLOOR - e * (2.0 + e))
        row = lax.broadcasted_iota(jnp.int32, (CHUNK, LANES), 0) + base
        own = row >= HALO
        A[at, :] = jnp.where(own, 1.0 + e, 1.0)
        B[at, :] = jnp.where(own, sc * (io * conv), 0.0)
        RO[at, :] = ro
        IO[at, :] = io
        SC[at, :] = sc
        q = ACC[at, pl.ds(LANES, LANES)].astype(BF16).astype(F32)
        cot = OG[at, :].astype(F32)
        t = jnp.tanh(GELU_A * (q + GELU_B * (q * q * q)))
        cdf = 0.5 * (1.0 + t)
        DG[at, :] = cot * (q * cdf)
        DGL[at, :] = cot * (cdf + 0.5 * q * (1.0 - t * t) * (GELU_A * (1.0 + 3.0 * GELU_B * (q * q))))
        return 0

    lax.fori_loop(0, nch, local, 0)

    STEP = 10

    def scan(i, carry):
        h, p, yb, q = carry
        for k in range(STEP):
            v = i * STEP + k
            fw, bw = pl.ds(v, 8, stride=SEG), pl.ds(SEG - 1 - v, 8, stride=SEG)
            a, b = A[fw, :], B[fw, :]
            HP[fw, :] = h
            PP[fw, :] = p
            h = a * h + b
            p = p * a
            a, g = A[bw, :], DG[bw, :]
            YN[bw, :] = yb
            QN[bw, :] = q
            yb = a * (g + yb)
            q = q * a
        return h, p, yb, q

    one, nil = jnp.ones((8, LANES), F32), jnp.zeros((8, LANES), F32)
    h, p, yb, q = lax.fori_loop(0, SEG // STEP, scan, (nil, one, nil, one))

    fa, fs, s_of, a_of = one[0:1], nil[0:1], [], []
    for k in range(8):
        s_of.append(fs)
        a_of.append(fa)
        fs = h[k : k + 1] + p[k : k + 1] * fs
        fa = fa * p[k : k + 1]
    ba, bs, t_of, c_of = one[0:1], nil[0:1], [None] * 8, [None] * 8
    for k in reversed(range(8)):
        t_of[k] = bs
        c_of[k] = ba
        bs = yb[k : k + 1] + q[k : k + 1] * bs
        ba = ba * q[k : k + 1]
    last, lead = HALO + rows - 1, 2 * HALO
    ls, fsg = last // SEG, lead // SEG
    la, lb = A[pl.ds(last, 1), :], B[pl.ds(last, 1), :]
    lp = PP[pl.ds(last, 1), :]
    out_a = la * lp * a_of[ls]
    out_s = la * (HP[pl.ds(last, 1), :] + lp * s_of[ls]) + lb
    ga, gg = A[pl.ds(lead, 1), :], DG[pl.ds(lead, 1), :]
    gq = QN[pl.ds(lead, 1), :]
    out_c = ga * gq * c_of[fsg]
    out_l = ga * (gg + YN[pl.ds(lead, 1), :] + gq * t_of[fsg])

    def put(ref, values):
        for k, value in enumerate(values):
            ref[pl.ds(k, 1), :] = value

    SUM[...] = nil
    put(SUM, (out_a, out_s, out_c, out_l))
    for d in far_y:
        send(SUM, RYC.at[y], ycs.at[d], ycr.at[y], y=lax.rem(y + d, NY))
    RYC[y] = SUM[...]

    def turn(i, _):
        GT[pl.ds(pl.multiple_of(i * LANES, LANES), LANES), :] = G[i, main, :].T
        return 0

    lax.fori_loop(0, NZ // 2, turn, 0)
    for d in range(1, NY):
        k = lax.rem(y + d, NY)
        arrived(RYC.at[k], ycs.at[d], ycr.at[k], c=1 - c)

    def compose(ref, count, place):
        fa, fs, fai, fsi = one[0:1], nil[0:1], one[0:1], nil[0:1]
        for k in range(count):
            a, s = ref[k, pl.ds(0, 1), :], ref[k, pl.ds(1, 1), :]
            fa, fs = fa * a, a * fs + s
            before = k < place
            fai, fsi = jnp.where(before, fa, fai), jnp.where(before, fs, fsi)
        ba, bs, bai, bsi = one[0:1], nil[0:1], one[0:1], nil[0:1]
        for k in reversed(range(count)):
            a, s = ref[k, pl.ds(2, 1), :], ref[k, pl.ds(3, 1), :]
            ba, bs = ba * a, a * bs + s
            after = k > place
            bai, bsi = jnp.where(after, ba, bai), jnp.where(after, bs, bsi)
        return (fa, fs, ba, bs), (fai, fsi, bai, bsi)

    total, inside = compose(RYC, NY, y)
    SUMZ[...] = nil
    put(SUMZ, total)
    for d in far_z:
        send(SUMZ, RZC.at[z], zcs.at[d], zcr.at[z], z=lax.rem(z + d, NZ))
    RZC[z] = SUMZ[...]
    lax.fori_loop(NZ // 2, NZ, turn, 0)
    for d in range(1, NZ):
        k = lax.rem(z + d, NZ)
        arrived(RZC.at[k], zcs.at[d], zcr.at[k], c=1 - c)
    _, outer = compose(RZC, NZ, z)
    carry_s = inside[1] + inside[0] * outer[1]
    carry_g = inside[3] + inside[2] * outer[3]
    put(CF, [s_of[k] + a_of[k] * carry_s for k in range(8)])
    put(CB, [t_of[k] + c_of[k] * carry_g for k in range(8)])
    cf, cb = CF[...], CB[...]

    def finish(i, _):
        for k in range(STEP):
            at = pl.ds(i * STEP + k, 8, stride=SEG)
            HP[at, :] = HP[at, :] + PP[at, :] * cf
            YN[at, :] = YN[at, :] + QN[at, :] * cb
        return 0

    lax.fori_loop(0, SEG // STEP, finish, 0)

    def gradients(i, _):
        base = pl.multiple_of(i * CHUNK, CHUNK)
        at = pl.ds(base, CHUNK)
        a, ro, io, sc = A[at, :], RO[at, :], IO[at, :], SC[at, :]
        conv = CV[at, :].astype(F32)
        decayed = a * HP[at, :]
        grad = DG[at, :] + YN[at, :]
        gated = io * conv
        DGL[at, :] = DGL[at, :] * (decayed + B[at, :])
        d_log = grad * (decayed - gated * a * a / sc)
        DR[at, pl.ds(0, LANES)] = (d_log * slope * ro * (1.0 - ro)).astype(BF16)
        gs = grad * sc
        DR[at, pl.ds(LANES, LANES)] = (gs * conv * io * (1.0 - io)).astype(BF16)
        DC[at, :] = gs * io
        return 0

    lax.fori_loop(0, nch, gradients, 0)
    dgate[...] = DGL[pl.ds(HALO, rows), :].astype(BF16)
    DC[pl.ds(0, R), :] += lax.dot_general(DR[...], gates, (((1,), (1,)), ((), ())), preferred_element_type=F32)

    WIDE = 96

    def unconvolve(i, _):
        base = pl.multiple_of(i * WIDE, WIDE)
        part = DC[pl.ds(base + HALO, WIDE + 8), :]
        total = taps[0] * part[:WIDE]
        for k in range(1, 4):
            total = total + taps[k] * pltpu.roll(part, WIDE + 8 - k, 0)[:WIDE]
        dproj[pl.ds(base, WIDE), :] = total.astype(BF16)
        return 0

    lax.fori_loop(0, rows // WIDE, unconvolve, 0)

    grad = dproj[...]
    share = LANES // NY
    per = NZ // 4
    for g in range(4):
        part = jnp.dot(GT[pl.ds(g * per * LANES, per * LANES), :], grad, preferred_element_type=F32).astype(BF16)
        for i in range(per):
            WS[:, g * per + i] = part[i * LANES : (i + 1) * LANES].reshape(NY, share, LANES)
        for d in far_y:
            k = lax.rem(y + d, NY)
            send(WS.at[k, pl.ds(g * per, per)], RY.at[y, pl.ds(g * per, per)], rys.at[g, d], ryr.at[g, y], y=k)
    for g in range(4):
        total = WS[y, pl.ds(g * per, per)].astype(F32)
        for d in range(1, NY):
            k = lax.rem(y + d, NY)
            arrived(RY.at[k, pl.ds(g * per, per)], rys.at[g, d], ryr.at[g, k], c=1 - c)
            total = total + RY[k, pl.ds(g * per, per)].astype(F32)
        VZ[pl.ds(g * per, per)] = total.astype(BF16)
    for d in far_z:
        k = lax.rem(z + d, NZ)
        send(VZ.at[k], RZ.at[z], rzs.at[d], rzr.at[z], z=k)
    total = VZ[z].astype(F32)
    for d in range(1, NZ):
        k = lax.rem(z + d, NZ)
        arrived(RZ.at[k], rzs.at[d], rzr.at[k], c=1 - c)
        total = total + RZ[k].astype(F32)
    dweight[...] = total
    for copy in pending:
        copy.wait_send()


def hand_over(a, b, c, a_out, b_out, c_out, sem):
    copies = [pltpu.make_async_copy(s, d, sem.at[k]) for k, (s, d) in enumerate(((a, a_out), (b, b_out), (c, c_out)))]
    for copy in copies:
        copy.start()
    for copy in copies:
        copy.wait()


def per_device(dims, tokens, proj_weight, gate_weight, conv_weight, recur_weight, input_weight, decay_param, out_grad):
    NZ, NY, NX, rows = dims
    R = rows + 2 * HALO
    share = LANES // NY
    vmem = pltpu.VMEM
    dma = pltpu.SemaphoreType.DMA
    flat = [vmem((R, LANES), F32)] * 11
    far, anywhere, inside = (pl.BlockSpec(memory_space=m) for m in (pltpu.HBM, pl.ANY, pltpu.VMEM))
    results = pl.pallas_call(
        functools.partial(kernel, dims),
        out_shape=(
            jax.ShapeDtypeStruct((rows, LANES), BF16),
            jax.ShapeDtypeStruct((rows, LANES), BF16),
            jax.ShapeDtypeStruct((share, LANES), F32),
        ),
        in_specs=[far] * 8,
        out_specs=(inside, inside, inside),
        scratch_shapes=[
            vmem((4 * NX, R, LANES), BF16),
            vmem(proj_weight.shape, BF16),
            vmem(gate_weight.shape, BF16),
            vmem((R, LANES), BF16),
            vmem((2, BLOCK, BLOCK), BF16),
            vmem((2, BLOCK, BLOCK), BF16),
            vmem((R, 2 * LANES), F32),
            vmem((R + 8, LANES), F32),
            vmem((R, LANES), BF16),
            vmem((R, 2 * LANES), F32),
            *flat,
            vmem((R, 2 * LANES), BF16),
            vmem((R + 8, LANES), F32),
            vmem((4 * NX * LANES, rows), BF16),
            vmem((8, LANES), F32),
            vmem((NY, 8, LANES), F32),
            vmem((8, LANES), F32),
            vmem((NZ, 8, LANES), F32),
            vmem((8, LANES), F32),
            vmem((8, LANES), F32),
            vmem((NY, NZ, share, LANES), BF16),
            vmem((NY, NZ, share, LANES), BF16),
            vmem((NZ, share, LANES), BF16),
            vmem((NZ, share, LANES), BF16),
            dma((9,)),
            dma((2 * NX,)),
            dma((2 * NX,)),
            dma((2 * NX,)),
            dma((2 * NX,)),
            dma((2,)),
            dma((14,)),
            dma((14,)),
            dma((NY,)),
            dma((NY,)),
            dma((NZ,)),
            dma((NZ,)),
            dma((4, NY)),
            dma((4, NY)),
            dma((NZ,)),
            dma((NZ,)),
            pltpu.SemaphoreType.REGULAR((5,)),
            vmem(conv_weight.shape, F32),
            vmem((decay_param.shape[0] // LANES, LANES), F32),
        ],
        compiler_params=pltpu.CompilerParams(collective_id=0, has_side_effects=True, vmem_limit_bytes=40 * 2**20),
    )(*(pltpu.with_memory_space_constraint(a, pltpu.HBM) for a in (
        tokens, proj_weight, gate_weight, conv_weight, recur_weight, input_weight,
        decay_param.reshape(-1, LANES), out_grad,
    )))
    return pl.pallas_call(
        hand_over,
        out_shape=[jax.ShapeDtypeStruct(r.shape, r.dtype) for r in results],
        in_specs=[inside] * 3,
        out_specs=[anywhere] * 3,
        scratch_shapes=[dma((3,))],
        compiler_params=pltpu.CompilerParams(vmem_limit_bytes=2**21),
    )(*results)


def solution(mesh):
    sizes = (16, 8, 4, 2)
    split = Mesh(mesh.devices.reshape(sizes), ("z", "y", "x", "c"))
    span, group = ("z", "y"), ("x", "c")
    placed = (P(span, group), P(None, group), P(None, group), P(), P(), P(), P(), P(span, group))

    def step(*args):
        return per_device((*sizes[:3], args[0].shape[0]), *args)

    return jax.shard_map(
        step,
        mesh=split,
        in_specs=placed,
        out_specs=(P(span, group), P(span, group), P(span, group)),
        check_vma=False,
    )
```

```python
import functools

import jax
import jax.numpy as jnp
from jax import lax
from jax.experimental import pallas as pl
from jax.experimental.pallas import tpu as pltpu
from jax.sharding import Mesh
from jax.sharding import PartitionSpec as P

MESH = pl.DeviceIdType.MESH
F32 = jnp.float32
BF16 = jnp.bfloat16
BLOCK = 64
HALO = 16
LANES = 128
RATE = 8.0
FLOOR = 0.0001
GELU_A = 0.7978845608028654
GELU_B = 0.044715
CHUNK = 80


def small_expm1(x):
    p = 1.0 / 5040.0
    for c in (1.0 / 720.0, 1.0 / 120.0, 1.0 / 24.0, 1.0 / 6.0, 0.5, 1.0):
        p = p * x + c
    return p * x


def small_log1p(u):
    p = -1.0 / 6.0
    for c in (1.0 / 5.0, -1.0 / 4.0, 1.0 / 3.0, -0.5, 1.0):
        p = p * u + c
    return p * u


def kernel(
    dims, tok, pw, gw, cw_far, rw, iw, dp_far, og, dproj, dgate, dweight,
    G, WP, WG, OG, RW, IW, ACC, PJ, CV, PRE, A, B, DG, RO, IO, SC, DGL, HP, PP, YN, QN, DR, DC,
    GT, SUM, RYC, SUMZ, RZC, CF, CB, WS, RY, VZ, RZ,
    lsem, hps, hpr, hns, hnr, ogs, ags, agr, ycs, ycr, zcs, zcr, rys, ryr, rzs, rzr, met, cw, dp,
):
    NZ, NY, NX, rows = dims
    R = rows + 2 * HALO
    SEG = R // 8
    nch = R // CHUNK
    z, y, x, c = (lax.axis_index(n) for n in ("z", "y", "x", "c"))
    sp = z * NY + y
    nsp = NZ * NY
    tp = x * 2 + c
    nxt, prv = lax.rem(sp + 1, nsp), lax.rem(sp + nsp - 1, nsp)
    nz, ny = nxt // NY, lax.rem(nxt, NY)
    pz, py = prv // NY, lax.rem(prv, NY)
    left, right, opp = lax.rem(x + NX - 1, NX), lax.rem(x + 1, NX), lax.rem(x + 2, NX)

    loads = [
        pltpu.make_async_copy(tok.at[:, pl.ds(h * LANES, LANES)], G.at[2 * tp + h, pl.ds(HALO, rows)], lsem.at[h])
        for h in range(2)
    ]
    loads += [
        pltpu.make_async_copy(pw, WP, lsem.at[2]),
        pltpu.make_async_copy(gw, WG, lsem.at[3]),
        pltpu.make_async_copy(og, OG.at[pl.ds(HALO, rows)], lsem.at[4]),
        pltpu.make_async_copy(rw.at[pl.ds(2 * tp, 2)], RW, lsem.at[5]),
        pltpu.make_async_copy(iw.at[pl.ds(2 * tp, 2)], IW, lsem.at[6]),
        pltpu.make_async_copy(cw_far, cw, lsem.at[7]),
        pltpu.make_async_copy(dp_far, dp, lsem.at[8]),
    ]
    for copy in loads:
        copy.start()

    barrier = pltpu.get_barrier_semaphore()

    def greet(**where):
        pl.semaphore_signal(barrier, inc=1, device_id=where, device_id_type=MESH)

    greet(c=1 - c)
    greet(x=left)
    greet(x=right)
    for k in range(NX):
        for d in range(2):
            greet(z=nz, y=ny, x=k, c=d)
            greet(z=pz, y=py, x=k, c=d)
    for d in (1, NY - 1):
        greet(y=lax.rem(y + d, NY))
    for d in (1, NZ - 1):
        greet(z=lax.rem(z + d, NZ))
    pl.semaphore_wait(barrier, 3 + 4 * NX + 4)

    def tell(sem, **where):
        pl.semaphore_signal(met.at[sem], inc=1, device_id=where, device_id_type=MESH)

    def tell_y(sem, d):
        tell(sem, y=lax.rem(y + d, NY))
        tell(sem, y=lax.rem(y + NY - d, NY))

    def tell_z(sem, d):
        tell(sem, z=lax.rem(z + d, NZ))
        tell(sem, z=lax.rem(z + NZ - d, NZ))

    far_y = sorted(range(1, NY), key=lambda d: -min(d, NY - d))
    far_z = sorted(range(1, NZ), key=lambda d: -min(d, NZ - d))
    pending = []

    def send(src, dst, ssem, rsem, **where):
        copy = pltpu.make_async_remote_copy(
            src_ref=src, dst_ref=dst, send_sem=ssem, recv_sem=rsem, device_id=where, device_id_type=MESH
        )
        copy.start()
        pending.append(copy)

    def arrived(dst, ssem, rsem, **where):
        pltpu.make_async_remote_copy(
            src_ref=dst, dst_ref=dst, send_sem=ssem, recv_sem=rsem, device_id=where, device_id_type=MESH
        ).wait_recv()

    loads[0].wait()
    loads[1].wait()
    mine = 2 * tp
    main = pl.ds(HALO, rows)
    for k in range(NX):
        for d in range(2):
            n = 2 * k + d
            send(G.at[pl.ds(mine, 2), pl.ds(rows, HALO)], G.at[pl.ds(mine, 2), pl.ds(0, HALO)],
                 hps.at[n], hpr.at[tp], z=nz, y=ny, x=k, c=d)
            send(G.at[pl.ds(mine, 2), pl.ds(HALO, HALO)], G.at[pl.ds(mine, 2), pl.ds(HALO + rows, HALO)],
                 hns.at[n], hnr.at[tp], z=pz, y=py, x=k, c=d)

    def piece(xx, cc, h):
        return 4 * xx + 2 * cc + h

    def give(i, sem, **where):
        send(G.at[i, main], G.at[i, main], ags.at[sem], agr.at[sem], **where)

    def got(i, sem):
        arrived(G.at[i, main], ags.at[sem], agr.at[sem], c=1 - c)

    p0, p1 = piece(x, c, 0), piece(x, c, 1)
    give(p0, 0, x=right)
    give(p1, 1, x=left)
    give(p1, 2, x=right)
    give(p0, 3, x=left)
    give(p0, 6, c=1 - c)
    give(p1, 7, c=1 - c)
    loads[4].wait()
    send(OG.at[pl.ds(HALO, HALO)], OG.at[pl.ds(HALO + rows, HALO)], ogs.at[0], ogs.at[1], z=pz, y=py)
    tell_y(0, 1)
    tell_z(1, 1)
    for k in (2, 3, 5, 6, 7, 8):
        loads[k].wait()

    OG[pl.ds(0, HALO), :] = jnp.zeros((HALO, LANES), BF16)
    PJ[pl.ds(0, 8), :] = jnp.zeros((8, LANES), F32)
    DC[pl.ds(R, 8), :] = jnp.zeros((8, LANES), F32)
    slope = -RATE * small_log1p(jnp.exp(-dp[pl.ds(tp, 1), :]))
    taps = [cw[pl.ds(k, 1), pl.ds(pl.multiple_of(tp * LANES, LANES), LANES)] for k in range(4)]
    zero = jnp.zeros((BLOCK, BLOCK), BF16)
    gates = jnp.concatenate(
        [
            jnp.concatenate([RW[0], zero, IW[0], zero], axis=1),
            jnp.concatenate([zero, RW[1], zero, IW[1]], axis=1),
        ],
        axis=0,
    )

    for n in range(2 * NX):
        arrived(G.at[pl.ds(2 * n, 2), pl.ds(0, HALO)], hps.at[n], hpr.at[n], c=1 - c)
        arrived(G.at[pl.ds(2 * n, 2), pl.ds(HALO + rows, HALO)], hns.at[n], hnr.at[n], c=1 - c)
    arrived(OG.at[pl.ds(HALO + rows, HALO)], ogs.at[0], ogs.at[1], c=1 - c)

    @pl.when(sp == 0)
    def _():
        G[:, pl.ds(0, HALO), :] = jnp.zeros((4 * NX, HALO, LANES), BF16)

    @pl.when(sp == nsp - 1)
    def _():
        G[:, pl.ds(HALO + rows, HALO), :] = jnp.zeros((4 * NX, HALO, LANES), BF16)
        OG[pl.ds(HALO + rows, HALO), :] = jnp.zeros((HALO, LANES), BF16)

    def multiply(i0, i1, first=False):
        def half(i):
            at = pl.ds(pl.multiple_of(i * LANES, LANES), LANES)
            return jnp.concatenate([WP[at, :], WG[at, :]], axis=1)

        rhs = jnp.concatenate([half(i0), half(i1)], axis=0)
        lhs = jnp.concatenate([G[i0], G[i1]], axis=1)
        out = jnp.dot(lhs, rhs, preferred_element_type=F32)
        if first:
            ACC[...] = out
        else:
            ACC[...] += out

    pl.semaphore_wait(met.at[0], 2)
    pl.semaphore_wait(met.at[1], 2)
    tell_y(2, 2)
    tell_z(3, 2)
    multiply(p0, p1, True)
    got(piece(x, 1 - c, 0), 6)
    got(piece(x, 1 - c, 1), 7)
    multiply(piece(x, 1 - c, 0), piece(x, 1 - c, 1))

    l0, l1 = piece(left, c, 0), piece(left, c, 1)
    r0, r1 = piece(right, c, 0), piece(right, c, 1)
    o0, o1 = piece(opp, c, 0), piece(opp, c, 1)
    got(l0, 0)
    give(l0, 4, x=right)
    give(l0, 8, c=1 - c)
    got(r1, 1)
    give(r1, 5, x=left)
    give(r1, 9, c=1 - c)
    multiply(l0, r1)
    got(piece(left, 1 - c, 0), 8)
    got(piece(right, 1 - c, 1), 9)
    multiply(piece(left, 1 - c, 0), piece(right, 1 - c, 1))
    pl.semaphore_wait(met.at[2], 2)
    pl.semaphore_wait(met.at[3], 2)
    tell_z(4, 4)
    got(l1, 2)
    give(l1, 10, c=1 - c)
    got(r0, 3)
    give(r0, 11, c=1 - c)
    multiply(l1, r0)
    got(piece(left, 1 - c, 1), 10)
    got(piece(right, 1 - c, 0), 11)
    multiply(piece(left, 1 - c, 1), piece(right, 1 - c, 0))
    pl.semaphore_wait(met.at[4], 2)
    got(o0, 4)
    give(o0, 12, c=1 - c)
    got(o1, 5)
    give(o1, 13, c=1 - c)
    multiply(o0, o1)
    got(piece(opp, 1 - c, 0), 12)
    got(piece(opp, 1 - c, 1), 13)
    multiply(piece(opp, 1 - c, 0), piece(opp, 1 - c, 1))

    PJ[pl.ds(8, R), :] = ACC[:, pl.ds(0, LANES)].astype(BF16).astype(F32)

    def convolve(i, _):
        base = pl.multiple_of(i * CHUNK, CHUNK)
        part = PJ[pl.ds(base, CHUNK + 8), :]
        total = taps[0] * part[8:]
        for k in range(1, 4):
            total = total + taps[k] * pltpu.roll(part, k, 0)[8:]
        CV[pl.ds(base, CHUNK), :] = total.astype(BF16)
        return 0

    lax.fori_loop(0, nch, convolve, 0)
    PRE[...] = jnp.dot(CV[...], gates, preferred_element_type=F32)

    def local(i, _):
        base = pl.multiple_of(i * CHUNK, CHUNK)
        at = pl.ds(base, CHUNK)
        ro = jax.nn.sigmoid(PRE[at, pl.ds(0, LANES)])
        io = jax.nn.sigmoid(PRE[at, pl.ds(LANES, LANES)])
        conv = CV[at, :].astype(F32)
        e = small_expm1(slope * ro)
        sc = jnp.sqrt(FLOOR - e * (2.0 + e))
        row = lax.broadcasted_iota(jnp.int32, (CHUNK, LANES), 0) + base
        own = row >= HALO
        A[at, :] = jnp.where(own, 1.0 + e, 1.0)
        B[at, :] = jnp.where(own, sc * (io * conv), 0.0)
        RO[at, :] = ro
        IO[at, :] = io
        SC[at, :] = sc
        q = ACC[at, pl.ds(LANES, LANES)].astype(BF16).astype(F32)
        cot = OG[at, :].astype(F32)
        t = jnp.tanh(GELU_A * (q + GELU_B * (q * q * q)))
        cdf = 0.5 * (1.0 + t)
        DG[at, :] = cot * (q * cdf)
        DGL[at, :] = t
        return 0

    lax.fori_loop(0, nch, local, 0)

    STEP = 10

    def scan(i, carry):
        h, p, yb, q = carry
        for k in range(STEP):
            v = i * STEP + k
            fw, bw = pl.ds(v, 8, stride=SEG), pl.ds(SEG - 1 - v, 8, stride=SEG)
            a, b = A[fw, :], B[fw, :]
            HP[fw, :] = h
            PP[fw, :] = p
            h = a * h + b
            p = p * a
            a, g = A[bw, :], DG[bw, :]
            YN[bw, :] = yb
            QN[bw, :] = q
            yb = a * (g + yb)
            q = q * a
        return h, p, yb, q

    one, nil = jnp.ones((8, LANES), F32), jnp.zeros((8, LANES), F32)
    h, p, yb, q = lax.fori_loop(0, SEG // STEP, scan, (nil, one, nil, one))

    fa, fs, s_of, a_of = one[0:1], nil[0:1], [], []
    for k in range(8):
        s_of.append(fs)
        a_of.append(fa)
        fs = h[k : k + 1] + p[k : k + 1] * fs
        fa = fa * p[k : k + 1]
    ba, bs, t_of, c_of = one[0:1], nil[0:1], [None] * 8, [None] * 8
    for k in reversed(range(8)):
        t_of[k] = bs
        c_of[k] = ba
        bs = yb[k : k + 1] + q[k : k + 1] * bs
        ba = ba * q[k : k + 1]
    last, lead = HALO + rows - 1, 2 * HALO
    ls, fsg = last // SEG, lead // SEG
    la, lb = A[pl.ds(last, 1), :], B[pl.ds(last, 1), :]
    lp = PP[pl.ds(last, 1), :]
    out_a = la * lp * a_of[ls]
    out_s = la * (HP[pl.ds(last, 1), :] + lp * s_of[ls]) + lb
    ga, gg = A[pl.ds(lead, 1), :], DG[pl.ds(lead, 1), :]
    gq = QN[pl.ds(lead, 1), :]
    out_c = ga * gq * c_of[fsg]
    out_l = ga * (gg + YN[pl.ds(lead, 1), :] + gq * t_of[fsg])

    def put(ref, values):
        for k, value in enumerate(values):
            ref[pl.ds(k, 1), :] = value

    share = LANES // NY
    SUM[...] = nil
    put(SUM, (out_a, out_s, out_c, out_l))
    for d in far_y:
        send(SUM, RYC.at[y], ycs.at[d], ycr.at[y], y=lax.rem(y + d, NY))
    RYC[y] = SUM[...]

    def factors(i, _):
        at = pl.ds(pl.multiple_of(i * CHUNK, CHUNK), CHUNK)
        a, ro, io, sc = A[at, :], RO[at, :], IO[at, :], SC[at, :]
        conv = CV[at, :].astype(F32)
        q = ACC[at, pl.ds(LANES, LANES)].astype(BF16).astype(F32)
        t = DGL[at, :]
        slant = 0.5 * (1.0 + t) + 0.5 * q * (1.0 - t * t) * (GELU_A * (1.0 + 3.0 * GELU_B * (q * q)))
        DGL[at, :] = OG[at, :].astype(F32) * slant
        both = sc * io
        PRE[at, pl.ds(0, LANES)] = (io * conv) * a * a / sc
        RO[at, :] = slope * ro * (1.0 - ro)
        IO[at, :] = both
        SC[at, :] = both * conv * (1.0 - io)
        return 0

    lax.fori_loop(0, nch, factors, 0)

    def turn(i, _):
        GT[:, i] = G[i, main, :].T.reshape(NY, share, rows)
        return 0

    lax.fori_loop(0, NZ // 2, turn, 0)
    for d in range(1, NY):
        k = lax.rem(y + d, NY)
        arrived(RYC.at[k], ycs.at[d], ycr.at[k], c=1 - c)

    def compose(ref, count, place):
        fa, fs, fai, fsi = one[0:1], nil[0:1], one[0:1], nil[0:1]
        for k in range(count):
            a, s = ref[k, pl.ds(0, 1), :], ref[k, pl.ds(1, 1), :]
            fa, fs = fa * a, a * fs + s
            before = k < place
            fai, fsi = jnp.where(before, fa, fai), jnp.where(before, fs, fsi)
        ba, bs, bai, bsi = one[0:1], nil[0:1], one[0:1], nil[0:1]
        for k in reversed(range(count)):
            a, s = ref[k, pl.ds(2, 1), :], ref[k, pl.ds(3, 1), :]
            ba, bs = ba * a, a * bs + s
            after = k > place
            bai, bsi = jnp.where(after, ba, bai), jnp.where(after, bs, bsi)
        return (fa, fs, ba, bs), (fai, fsi, bai, bsi)

    total, inside = compose(RYC, NY, y)
    SUMZ[...] = nil
    put(SUMZ, total)
    for d in far_z:
        send(SUMZ, RZC.at[z], zcs.at[d], zcr.at[z], z=lax.rem(z + d, NZ))
    RZC[z] = SUMZ[...]
    lax.fori_loop(NZ // 2, NZ, turn, 0)
    for d in range(1, NZ):
        k = lax.rem(z + d, NZ)
        arrived(RZC.at[k], zcs.at[d], zcr.at[k], c=1 - c)
    _, outer = compose(RZC, NZ, z)
    carry_s = inside[1] + inside[0] * outer[1]
    carry_g = inside[3] + inside[2] * outer[3]
    put(CF, [s_of[k] + a_of[k] * carry_s for k in range(8)])
    put(CB, [t_of[k] + c_of[k] * carry_g for k in range(8)])
    cf, cb = CF[...], CB[...]

    def finish(i, _):
        for k in range(STEP):
            at = pl.ds(i * STEP + k, 8, stride=SEG)
            HP[at, :] = HP[at, :] + PP[at, :] * cf
            YN[at, :] = YN[at, :] + QN[at, :] * cb
        return 0

    lax.fori_loop(0, SEG // STEP, finish, 0)

    def gradients(i, _):
        base = pl.multiple_of(i * CHUNK, CHUNK)
        at = pl.ds(base, CHUNK)
        grad = DG[at, :] + YN[at, :]
        d_log = grad * (A[at, :] * HP[at, :] - PRE[at, pl.ds(0, LANES)])
        DR[at, pl.ds(0, LANES)] = (d_log * RO[at, :]).astype(BF16)
        DR[at, pl.ds(LANES, LANES)] = (grad * SC[at, :]).astype(BF16)
        DC[at, :] = grad * IO[at, :]
        return 0

    lax.fori_loop(0, nch, gradients, 0)
    DC[pl.ds(0, R), :] += lax.dot_general(DR[...], gates, (((1,), (1,)), ((), ())), preferred_element_type=F32)

    WIDE = 96

    def unconvolve(i, _):
        base = pl.multiple_of(i * WIDE, WIDE)
        part = DC[pl.ds(base + HALO, WIDE + 8), :]
        total = taps[0] * part[:WIDE]
        for k in range(1, 4):
            total = total + taps[k] * pltpu.roll(part, WIDE + 8 - k, 0)[:WIDE]
        dproj[pl.ds(base, WIDE), :] = total.astype(BF16)
        return 0

    lax.fori_loop(0, rows // WIDE, unconvolve, 0)

    grad = dproj[...]
    half = NZ // 2
    sides = [pl.ds(0, half), pl.ds(half, half)]

    def along(d):
        return lax.rem(y + NY + d, NY)

    def partial(d):
        k = along(d)
        part = jnp.dot(GT[k].reshape(NZ * share, rows), grad, preferred_element_type=F32)
        WS[k] = part.astype(BF16).reshape(NZ, share, LANES)
        return k

    def hop(k, h, slot, d):
        send(WS.at[k, sides[h]], RY.at[slot, sides[h]], rys.at[slot, h], ryr.at[slot, h], y=along(d))

    def landed(slot, h):
        arrived(RY.at[slot, sides[h]], rys.at[slot, h], ryr.at[slot, h], c=1 - c)

    def add(k, h, slot):
        landed(slot, h)
        WS[k, sides[h]] = (WS[k, sides[h]].astype(F32) + RY[slot, sides[h]].astype(F32)).astype(BF16)

    k = partial(4)
    hop(k, 0, 0, 2)
    hop(k, 1, 0, -2)
    k = partial(3)
    hop(k, 0, 1, 2)
    hop(k, 1, 1, 2)
    k = partial(-3)
    hop(k, 0, 2, -2)
    hop(k, 1, 2, -2)
    hop(partial(2), 1, 3, 2)
    hop(partial(-2), 0, 4, -2)
    partial(1)
    partial(-1)
    partial(0)
    dgate[...] = (DGL[pl.ds(HALO, rows), :] * (A[pl.ds(HALO, rows), :] * HP[pl.ds(HALO, rows), :] + B[pl.ds(HALO, rows), :])).astype(BF16)
    add(along(2), 0, 0)
    hop(along(2), 0, 3, 2)
    for h in range(2):
        add(along(1), h, 1)
        hop(along(1), h, 5, 1)
        add(along(-1), h, 2)
        hop(along(-1), h, 6, -1)
    add(along(-2), 1, 0)
    hop(along(-2), 1, 4, -2)
    for h in range(2):
        total = WS[y, sides[h]].astype(F32)
        for slot in (3, 4, 5, 6):
            landed(slot, h)
            total = total + RY[slot, sides[h]].astype(F32)
        VZ[sides[h]] = total.astype(BF16)
    for d in far_z:
        k = lax.rem(z + d, NZ)
        send(VZ.at[k], RZ.at[z], rzs.at[d], rzr.at[z], z=k)
    total = VZ[z].astype(F32)
    for d in range(1, NZ):
        k = lax.rem(z + d, NZ)
        arrived(RZ.at[k], rzs.at[d], rzr.at[k], c=1 - c)
        total = total + RZ[k].astype(F32)
    dweight[...] = total
    for copy in pending:
        copy.wait_send()


def hand_over(a, b, c, a_out, b_out, c_out, sem):
    copies = [pltpu.make_async_copy(s, d, sem.at[k]) for k, (s, d) in enumerate(((a, a_out), (b, b_out), (c, c_out)))]
    for copy in copies:
        copy.start()
    for copy in copies:
        copy.wait()


def per_device(dims, tokens, proj_weight, gate_weight, conv_weight, recur_weight, input_weight, decay_param, out_grad):
    NZ, NY, NX, rows = dims
    R = rows + 2 * HALO
    share = LANES // NY
    vmem = pltpu.VMEM
    dma = pltpu.SemaphoreType.DMA
    flat = [vmem((R, LANES), F32)] * 11
    far, anywhere, inside = (pl.BlockSpec(memory_space=m) for m in (pltpu.HBM, pl.ANY, pltpu.VMEM))
    results = pl.pallas_call(
        functools.partial(kernel, dims),
        out_shape=(
            jax.ShapeDtypeStruct((rows, LANES), BF16),
            jax.ShapeDtypeStruct((rows, LANES), BF16),
            jax.ShapeDtypeStruct((share, LANES), F32),
        ),
        in_specs=[far] * 8,
        out_specs=(inside, inside, inside),
        scratch_shapes=[
            vmem((4 * NX, R, LANES), BF16),
            vmem(proj_weight.shape, BF16),
            vmem(gate_weight.shape, BF16),
            vmem((R, LANES), BF16),
            vmem((2, BLOCK, BLOCK), BF16),
            vmem((2, BLOCK, BLOCK), BF16),
            vmem((R, 2 * LANES), F32),
            vmem((R + 8, LANES), F32),
            vmem((R, LANES), BF16),
            vmem((R, 2 * LANES), F32),
            *flat,
            vmem((R, 2 * LANES), BF16),
            vmem((R + 8, LANES), F32),
            vmem((NY, NZ, share, rows), BF16),
            vmem((8, LANES), F32),
            vmem((NY, 8, LANES), F32),
            vmem((8, LANES), F32),
            vmem((NZ, 8, LANES), F32),
            vmem((8, LANES), F32),
            vmem((8, LANES), F32),
            vmem((NY, NZ, share, LANES), BF16),
            vmem((NY, NZ, share, LANES), BF16),
            vmem((NZ, share, LANES), BF16),
            vmem((NZ, share, LANES), BF16),
            dma((9,)),
            dma((2 * NX,)),
            dma((2 * NX,)),
            dma((2 * NX,)),
            dma((2 * NX,)),
            dma((2,)),
            dma((14,)),
            dma((14,)),
            dma((NY,)),
            dma((NY,)),
            dma((NZ,)),
            dma((NZ,)),
            dma((7, 2)),
            dma((7, 2)),
            dma((NZ,)),
            dma((NZ,)),
            pltpu.SemaphoreType.REGULAR((5,)),
            vmem(conv_weight.shape, F32),
            vmem((decay_param.shape[0] // LANES, LANES), F32),
        ],
        compiler_params=pltpu.CompilerParams(collective_id=0, has_side_effects=True, vmem_limit_bytes=40 * 2**20),
    )(*(pltpu.with_memory_space_constraint(a, pltpu.HBM) for a in (
        tokens, proj_weight, gate_weight, conv_weight, recur_weight, input_weight,
        decay_param.reshape(-1, LANES), out_grad,
    )))
    return pl.pallas_call(
        hand_over,
        out_shape=[jax.ShapeDtypeStruct(r.shape, r.dtype) for r in results],
        in_specs=[inside] * 3,
        out_specs=[anywhere] * 3,
        scratch_shapes=[dma((3,))],
        compiler_params=pltpu.CompilerParams(vmem_limit_bytes=2**21),
    )(*results)


def solution(mesh):
    sizes = (16, 8, 4, 2)
    split = Mesh(mesh.devices.reshape(sizes), ("z", "y", "x", "c"))
    span, group = ("z", "y"), ("x", "c")
    placed = (P(span, group), P(None, group), P(None, group), P(), P(), P(), P(), P(span, group))

    def step(*args):
        return per_device((*sizes[:3], args[0].shape[0]), *args)

    return jax.shard_map(
        step,
        mesh=split,
        in_specs=placed,
        out_specs=(P(span, group), P(span, group), P(span, group)),
        check_vma=False,
    )
```

```python
import functools

import jax
import jax.numpy as jnp
from jax import lax
from jax.experimental import pallas as pl
from jax.experimental.pallas import tpu as pltpu
from jax.sharding import Mesh
from jax.sharding import PartitionSpec as P

MESH = pl.DeviceIdType.MESH
F32 = jnp.float32
BF16 = jnp.bfloat16
BLOCK = 64
HALO = 16
LANES = 128
RATE = 8.0
FLOOR = 0.0001
GELU_A = 0.7978845608028654
GELU_B = 0.044715
CHUNK = 80


def small_expm1(x):
    p = 1.0 / 5040.0
    for c in (1.0 / 720.0, 1.0 / 120.0, 1.0 / 24.0, 1.0 / 6.0, 0.5, 1.0):
        p = p * x + c
    return p * x


def small_log1p(u):
    p = -1.0 / 6.0
    for c in (1.0 / 5.0, -1.0 / 4.0, 1.0 / 3.0, -0.5, 1.0):
        p = p * u + c
    return p * u


def kernel(
    dims, tok, pw, gw, cw_far, rw, iw, dp_far, og, dproj, dgate, dweight,
    G, WP, WG, OG, RW, IW, ACC, PJ, CV, PRE, A, B, DG, RO, IO, SC, DGL, HP, PP, YN, QN, DR, DC,
    GT, SUM, RYC, SUMZ, RZC, CF, CB, WS, RY, VZ, RZ,
    lsem, hys, hyr, hxs, hxr, ogs, ags, agr, ycs, ycr, zcs, zcr, rys, ryr, rzs, rzr, met, cw, dp,
):
    NZ, NY, NX, rows = dims
    R = rows + 2 * HALO
    SEG = R // 8
    nch = R // CHUNK
    z, y, x, c = (lax.axis_index(n) for n in ("z", "y", "x", "c"))
    sp = z * NY + y
    nsp = NZ * NY
    tp = x * 2 + c
    nxt, prv = lax.rem(sp + 1, nsp), lax.rem(sp + nsp - 1, nsp)
    nz, ny = nxt // NY, lax.rem(nxt, NY)
    pz, py = prv // NY, lax.rem(prv, NY)
    left, right, opp = lax.rem(x + NX - 1, NX), lax.rem(x + 1, NX), lax.rem(x + 2, NX)

    loads = [
        pltpu.make_async_copy(tok.at[:, pl.ds(h * LANES, LANES)], G.at[2 * tp + h, pl.ds(HALO, rows)], lsem.at[h])
        for h in range(2)
    ]
    loads += [
        pltpu.make_async_copy(pw, WP, lsem.at[2]),
        pltpu.make_async_copy(gw, WG, lsem.at[3]),
        pltpu.make_async_copy(og, OG.at[pl.ds(HALO, rows)], lsem.at[4]),
        pltpu.make_async_copy(rw.at[pl.ds(2 * tp, 2)], RW, lsem.at[5]),
        pltpu.make_async_copy(iw.at[pl.ds(2 * tp, 2)], IW, lsem.at[6]),
        pltpu.make_async_copy(cw_far, cw, lsem.at[7]),
        pltpu.make_async_copy(dp_far, dp, lsem.at[8]),
    ]
    for copy in loads:
        copy.start()

    barrier = pltpu.get_barrier_semaphore()

    def greet(**where):
        pl.semaphore_signal(barrier, inc=1, device_id=where, device_id_type=MESH)

    greet(c=1 - c)
    greet(x=left)
    greet(x=right)
    greet(z=nz, y=ny)
    greet(z=pz, y=py)
    for d in (1, NY - 1):
        greet(y=lax.rem(y + d, NY))
    for d in (1, NZ - 1):
        greet(z=lax.rem(z + d, NZ))
    pl.semaphore_wait(barrier, 9)

    def tell(sem, **where):
        pl.semaphore_signal(met.at[sem], inc=1, device_id=where, device_id_type=MESH)

    def tell_y(sem, d):
        tell(sem, y=lax.rem(y + d, NY))
        tell(sem, y=lax.rem(y + NY - d, NY))

    def tell_z(sem, d):
        tell(sem, z=lax.rem(z + d, NZ))
        tell(sem, z=lax.rem(z + NZ - d, NZ))

    far_y = sorted(range(1, NY), key=lambda d: -min(d, NY - d))
    far_z = sorted(range(1, NZ), key=lambda d: -min(d, NZ - d))
    pending = []

    def send(src, dst, ssem, rsem, **where):
        copy = pltpu.make_async_remote_copy(
            src_ref=src, dst_ref=dst, send_sem=ssem, recv_sem=rsem, device_id=where, device_id_type=MESH
        )
        copy.start()
        pending.append(copy)

    def arrived(dst, ssem, rsem, **where):
        pltpu.make_async_remote_copy(
            src_ref=dst, dst_ref=dst, send_sem=ssem, recv_sem=rsem, device_id=where, device_id_type=MESH
        ).wait_recv()

    loads[0].wait()
    loads[1].wait()
    mine = 2 * tp
    main = pl.ds(HALO, rows)
    edges = (pl.ds(0, HALO), pl.ds(HALO + rows, HALO))
    send(G.at[pl.ds(mine, 2), pl.ds(rows, HALO)], G.at[pl.ds(mine, 2), edges[0]], hys.at[0], hyr.at[0], z=nz, y=ny)
    send(G.at[pl.ds(mine, 2), pl.ds(HALO, HALO)], G.at[pl.ds(mine, 2), edges[1]], hys.at[1], hyr.at[1], z=pz, y=py)

    def halo(xx, cc, k):
        return G.at[pl.ds(4 * xx + 2 * cc, 2), edges[k]]

    def pass_halo(xx, slot, k, **where):
        send(halo(xx, c, k), halo(xx, c, k), hxs.at[slot, k], hxr.at[slot, k], **where)

    def got_halo(xx, cc, slot, k):
        arrived(halo(xx, cc, k), hxs.at[slot, k], hxr.at[slot, k], c=1 - c)

    def piece(xx, cc, h):
        return 4 * xx + 2 * cc + h

    def give(i, sem, **where):
        send(G.at[i, main], G.at[i, main], ags.at[sem], agr.at[sem], **where)

    def got(i, sem):
        arrived(G.at[i, main], ags.at[sem], agr.at[sem], c=1 - c)

    p0, p1 = piece(x, c, 0), piece(x, c, 1)
    give(p0, 0, x=right)
    give(p1, 1, x=left)
    give(p0, 6, c=1 - c)
    give(p1, 7, c=1 - c)
    loads[4].wait()
    send(OG.at[pl.ds(HALO, HALO)], OG.at[pl.ds(HALO + rows, HALO)], ogs.at[0], ogs.at[1], z=pz, y=py)
    tell_y(0, 1)
    tell_z(1, 1)
    for k in (2, 3, 5, 6, 7, 8):
        loads[k].wait()

    OG[pl.ds(0, HALO), :] = jnp.zeros((HALO, LANES), BF16)
    PJ[pl.ds(0, 8), :] = jnp.zeros((8, LANES), F32)
    DC[pl.ds(R, 8), :] = jnp.zeros((8, LANES), F32)
    slope = -RATE * small_log1p(jnp.exp(-dp[pl.ds(tp, 1), :]))
    taps = [cw[pl.ds(k, 1), pl.ds(pl.multiple_of(tp * LANES, LANES), LANES)] for k in range(4)]
    zero = jnp.zeros((BLOCK, BLOCK), BF16)
    gates = jnp.concatenate(
        [
            jnp.concatenate([RW[0], zero, IW[0], zero], axis=1),
            jnp.concatenate([zero, RW[1], zero, IW[1]], axis=1),
        ],
        axis=0,
    )

    for k in range(2):
        arrived(halo(x, c, k), hys.at[k], hyr.at[k], c=1 - c)
        pass_halo(x, 0, k, x=right)
        pass_halo(x, 1, k, x=left)
        pass_halo(x, 3, k, c=1 - c)
    give(p1, 2, x=right)
    give(p0, 3, x=left)
    arrived(OG.at[pl.ds(HALO + rows, HALO)], ogs.at[0], ogs.at[1], c=1 - c)

    @pl.when(sp == nsp - 1)
    def _():
        OG[pl.ds(HALO + rows, HALO), :] = jnp.zeros((HALO, LANES), BF16)

    def multiply(i0, i1, first=False):
        def half(i):
            at = pl.ds(pl.multiple_of(i * LANES, LANES), LANES)
            return jnp.concatenate([WP[at, :], WG[at, :]], axis=1)

        rhs = jnp.concatenate([half(i0), half(i1)], axis=0)
        lhs = jnp.concatenate([G[i0], G[i1]], axis=1)
        out = jnp.dot(lhs, rhs, preferred_element_type=F32)
        if first:
            ACC[...] = out
        else:
            ACC[...] += out

    pl.semaphore_wait(met.at[0], 2)
    pl.semaphore_wait(met.at[1], 2)
    tell_y(2, 2)
    tell_z(3, 2)
    multiply(p0, p1, True)
    got(piece(x, 1 - c, 0), 6)
    got(piece(x, 1 - c, 1), 7)
    for k in range(2):
        got_halo(x, 1 - c, 3, k)
    multiply(piece(x, 1 - c, 0), piece(x, 1 - c, 1))

    l0, l1 = piece(left, c, 0), piece(left, c, 1)
    r0, r1 = piece(right, c, 0), piece(right, c, 1)
    o0, o1 = piece(opp, c, 0), piece(opp, c, 1)
    got(l0, 0)
    for k in range(2):
        got_halo(left, c, 0, k)
    pass_halo(left, 2, 0, x=right)
    give(l0, 4, x=right)
    give(l0, 8, c=1 - c)
    got(r1, 1)
    for k in range(2):
        got_halo(right, c, 1, k)
    pass_halo(right, 2, 1, x=left)
    give(r1, 5, x=left)
    give(r1, 9, c=1 - c)
    for k in range(2):
        pass_halo(left, 4, k, c=1 - c)
        pass_halo(right, 5, k, c=1 - c)
    multiply(l0, r1)
    got(piece(left, 1 - c, 0), 8)
    got(piece(right, 1 - c, 1), 9)
    for k in range(2):
        got_halo(left, 1 - c, 4, k)
        got_halo(right, 1 - c, 5, k)
    multiply(piece(left, 1 - c, 0), piece(right, 1 - c, 1))
    pl.semaphore_wait(met.at[2], 2)
    pl.semaphore_wait(met.at[3], 2)
    tell_z(4, 4)
    got(l1, 2)
    give(l1, 10, c=1 - c)
    got(r0, 3)
    give(r0, 11, c=1 - c)
    multiply(l1, r0)
    got(piece(left, 1 - c, 1), 10)
    got(piece(right, 1 - c, 0), 11)
    multiply(piece(left, 1 - c, 1), piece(right, 1 - c, 0))
    pl.semaphore_wait(met.at[4], 2)
    for k in range(2):
        got_halo(opp, c, 2, k)
        pass_halo(opp, 6, k, c=1 - c)
    got(o0, 4)
    give(o0, 12, c=1 - c)
    got(o1, 5)
    give(o1, 13, c=1 - c)
    multiply(o0, o1)
    got(piece(opp, 1 - c, 0), 12)
    got(piece(opp, 1 - c, 1), 13)
    for k in range(2):
        got_halo(opp, 1 - c, 6, k)
    multiply(piece(opp, 1 - c, 0), piece(opp, 1 - c, 1))

    PJ[pl.ds(8, R), :] = ACC[:, pl.ds(0, LANES)].astype(BF16).astype(F32)

    @pl.when(sp == 0)
    def _():
        PJ[pl.ds(8, HALO), :] = jnp.zeros((HALO, LANES), F32)

    def convolve(i, _):
        base = pl.multiple_of(i * CHUNK, CHUNK)
        part = PJ[pl.ds(base, CHUNK + 8), :]
        total = taps[0] * part[8:]
        for k in range(1, 4):
            total = total + taps[k] * pltpu.roll(part, k, 0)[8:]
        CV[pl.ds(base, CHUNK), :] = total.astype(BF16)
        return 0

    lax.fori_loop(0, nch, convolve, 0)
    PRE[...] = jnp.dot(CV[...], gates, preferred_element_type=F32)

    def local(i, _):
        base = pl.multiple_of(i * CHUNK, CHUNK)
        at = pl.ds(base, CHUNK)
        ro = jax.nn.sigmoid(PRE[at, pl.ds(0, LANES)])
        io = jax.nn.sigmoid(PRE[at, pl.ds(LANES, LANES)])
        conv = CV[at, :].astype(F32)
        e = small_expm1(slope * ro)
        sc = jnp.sqrt(FLOOR - e * (2.0 + e))
        row = lax.broadcasted_iota(jnp.int32, (CHUNK, LANES), 0) + base
        own = row >= HALO
        A[at, :] = jnp.where(own, 1.0 + e, 1.0)
        B[at, :] = jnp.where(own, sc * (io * conv), 0.0)
        RO[at, :] = ro
        IO[at, :] = io
        SC[at, :] = sc
        q = ACC[at, pl.ds(LANES, LANES)].astype(BF16).astype(F32)
        cot = OG[at, :].astype(F32)
        t = jnp.tanh(GELU_A * (q + GELU_B * (q * q * q)))
        cdf = 0.5 * (1.0 + t)
        DG[at, :] = cot * (q * cdf)
        DGL[at, :] = t
        return 0

    lax.fori_loop(0, nch, local, 0)

    STEP = 10

    def scan(i, carry):
        h, p, yb, q = carry
        for k in range(STEP):
            v = i * STEP + k
            fw, bw = pl.ds(v, 8, stride=SEG), pl.ds(SEG - 1 - v, 8, stride=SEG)
            a, b = A[fw, :], B[fw, :]
            HP[fw, :] = h
            PP[fw, :] = p
            h = a * h + b
            p = p * a
            a, g = A[bw, :], DG[bw, :]
            YN[bw, :] = yb
            QN[bw, :] = q
            yb = a * (g + yb)
            q = q * a
        return h, p, yb, q

    one, nil = jnp.ones((8, LANES), F32), jnp.zeros((8, LANES), F32)
    h, p, yb, q = lax.fori_loop(0, SEG // STEP, scan, (nil, one, nil, one))

    fa, fs, s_of, a_of = one[0:1], nil[0:1], [], []
    for k in range(8):
        s_of.append(fs)
        a_of.append(fa)
        fs = h[k : k + 1] + p[k : k + 1] * fs
        fa = fa * p[k : k + 1]
    ba, bs, t_of, c_of = one[0:1], nil[0:1], [None] * 8, [None] * 8
    for k in reversed(range(8)):
        t_of[k] = bs
        c_of[k] = ba
        bs = yb[k : k + 1] + q[k : k + 1] * bs
        ba = ba * q[k : k + 1]
    last, lead = HALO + rows - 1, 2 * HALO
    ls, fsg = last // SEG, lead // SEG
    la, lb = A[pl.ds(last, 1), :], B[pl.ds(last, 1), :]
    lp = PP[pl.ds(last, 1), :]
    out_a = la * lp * a_of[ls]
    out_s = la * (HP[pl.ds(last, 1), :] + lp * s_of[ls]) + lb
    ga, gg = A[pl.ds(lead, 1), :], DG[pl.ds(lead, 1), :]
    gq = QN[pl.ds(lead, 1), :]
    out_c = ga * gq * c_of[fsg]
    out_l = ga * (gg + YN[pl.ds(lead, 1), :] + gq * t_of[fsg])

    def put(ref, values):
        for k, value in enumerate(values):
            ref[pl.ds(k, 1), :] = value

    share = LANES // NY
    SUM[...] = nil
    put(SUM, (out_a, out_s, out_c, out_l))
    for d in far_y:
        send(SUM, RYC.at[y], ycs.at[d], ycr.at[y], y=lax.rem(y + d, NY))
    RYC[y] = SUM[...]

    def factors(i, _):
        at = pl.ds(pl.multiple_of(i * CHUNK, CHUNK), CHUNK)
        a, ro, io, sc = A[at, :], RO[at, :], IO[at, :], SC[at, :]
        conv = CV[at, :].astype(F32)
        q = ACC[at, pl.ds(LANES, LANES)].astype(BF16).astype(F32)
        t = DGL[at, :]
        slant = 0.5 * (1.0 + t) + 0.5 * q * (1.0 - t * t) * (GELU_A * (1.0 + 3.0 * GELU_B * (q * q)))
        DGL[at, :] = OG[at, :].astype(F32) * slant
        both = sc * io
        PRE[at, pl.ds(0, LANES)] = (io * conv) * a * a / sc
        RO[at, :] = slope * ro * (1.0 - ro)
        IO[at, :] = both
        SC[at, :] = both * conv * (1.0 - io)
        return 0

    lax.fori_loop(0, nch, factors, 0)

    def turn(i, _):
        GT[:, i] = G[i, main, :].T.reshape(NY, share, rows)
        return 0

    lax.fori_loop(0, NZ // 2, turn, 0)
    for d in range(1, NY):
        k = lax.rem(y + d, NY)
        arrived(RYC.at[k], ycs.at[d], ycr.at[k], c=1 - c)

    def compose(ref, count, place):
        fa, fs, fai, fsi = one[0:1], nil[0:1], one[0:1], nil[0:1]
        for k in range(count):
            a, s = ref[k, pl.ds(0, 1), :], ref[k, pl.ds(1, 1), :]
            fa, fs = fa * a, a * fs + s
            before = k < place
            fai, fsi = jnp.where(before, fa, fai), jnp.where(before, fs, fsi)
        ba, bs, bai, bsi = one[0:1], nil[0:1], one[0:1], nil[0:1]
        for k in reversed(range(count)):
            a, s = ref[k, pl.ds(2, 1), :], ref[k, pl.ds(3, 1), :]
            ba, bs = ba * a, a * bs + s
            after = k > place
            bai, bsi = jnp.where(after, ba, bai), jnp.where(after, bs, bsi)
        return (fa, fs, ba, bs), (fai, fsi, bai, bsi)

    total, inside = compose(RYC, NY, y)
    SUMZ[...] = nil
    put(SUMZ, total)
    for d in far_z:
        send(SUMZ, RZC.at[z], zcs.at[d], zcr.at[z], z=lax.rem(z + d, NZ))
    RZC[z] = SUMZ[...]
    lax.fori_loop(NZ // 2, NZ, turn, 0)
    for d in range(1, NZ):
        k = lax.rem(z + d, NZ)
        arrived(RZC.at[k], zcs.at[d], zcr.at[k], c=1 - c)
    _, outer = compose(RZC, NZ, z)
    carry_s = inside[1] + inside[0] * outer[1]
    carry_g = inside[3] + inside[2] * outer[3]
    put(CF, [s_of[k] + a_of[k] * carry_s for k in range(8)])
    put(CB, [t_of[k] + c_of[k] * carry_g for k in range(8)])
    cf, cb = CF[...], CB[...]

    def finish(i, _):
        for k in range(STEP):
            at = pl.ds(i * STEP + k, 8, stride=SEG)
            HP[at, :] = HP[at, :] + PP[at, :] * cf
            YN[at, :] = YN[at, :] + QN[at, :] * cb
        return 0

    lax.fori_loop(0, SEG // STEP, finish, 0)

    def gradients(i, _):
        base = pl.multiple_of(i * CHUNK, CHUNK)
        at = pl.ds(base, CHUNK)
        grad = DG[at, :] + YN[at, :]
        d_log = grad * (A[at, :] * HP[at, :] - PRE[at, pl.ds(0, LANES)])
        DR[at, pl.ds(0, LANES)] = (d_log * RO[at, :]).astype(BF16)
        DR[at, pl.ds(LANES, LANES)] = (grad * SC[at, :]).astype(BF16)
        DC[at, :] = grad * IO[at, :]
        return 0

    lax.fori_loop(0, nch, gradients, 0)
    DC[pl.ds(0, R), :] += lax.dot_general(DR[...], gates, (((1,), (1,)), ((), ())), preferred_element_type=F32)

    WIDE = 96

    def unconvolve(i, _):
        base = pl.multiple_of(i * WIDE, WIDE)
        part = DC[pl.ds(base + HALO, WIDE + 8), :]
        total = taps[0] * part[:WIDE]
        for k in range(1, 4):
            total = total + taps[k] * pltpu.roll(part, WIDE + 8 - k, 0)[:WIDE]
        dproj[pl.ds(base, WIDE), :] = total.astype(BF16)
        return 0

    lax.fori_loop(0, rows // WIDE, unconvolve, 0)

    grad = dproj[...]
    half = NZ // 2
    sides = [pl.ds(0, half), pl.ds(half, half)]

    def along(d):
        return lax.rem(y + NY + d, NY)

    def partial(d):
        k = along(d)
        part = jnp.dot(GT[k].reshape(NZ * share, rows), grad, preferred_element_type=F32)
        WS[k] = part.astype(BF16).reshape(NZ, share, LANES)
        return k

    def hop(k, h, slot, d):
        send(WS.at[k, sides[h]], RY.at[slot, sides[h]], rys.at[slot, h], ryr.at[slot, h], y=along(d))

    def landed(slot, h):
        arrived(RY.at[slot, sides[h]], rys.at[slot, h], ryr.at[slot, h], c=1 - c)

    def add(k, h, slot):
        landed(slot, h)
        WS[k, sides[h]] = (WS[k, sides[h]].astype(F32) + RY[slot, sides[h]].astype(F32)).astype(BF16)

    k = partial(4)
    hop(k, 0, 0, 2)
    hop(k, 1, 0, -2)
    k = partial(3)
    hop(k, 0, 1, 2)
    hop(k, 1, 1, 2)
    k = partial(-3)
    hop(k, 0, 2, -2)
    hop(k, 1, 2, -2)
    hop(partial(2), 1, 3, 2)
    hop(partial(-2), 0, 4, -2)
    partial(1)
    partial(-1)
    partial(0)
    dgate[...] = (DGL[pl.ds(HALO, rows), :] * (A[pl.ds(HALO, rows), :] * HP[pl.ds(HALO, rows), :] + B[pl.ds(HALO, rows), :])).astype(BF16)
    add(along(2), 0, 0)
    hop(along(2), 0, 3, 2)
    for h in range(2):
        add(along(1), h, 1)
        hop(along(1), h, 5, 1)
        add(along(-1), h, 2)
        hop(along(-1), h, 6, -1)
    add(along(-2), 1, 0)
    hop(along(-2), 1, 4, -2)
    for h in range(2):
        total = WS[y, sides[h]].astype(F32)
        for slot in (3, 4, 5, 6):
            landed(slot, h)
            total = total + RY[slot, sides[h]].astype(F32)
        VZ[sides[h]] = total.astype(BF16)
    for d in far_z:
        k = lax.rem(z + d, NZ)
        send(VZ.at[k], RZ.at[z], rzs.at[d], rzr.at[z], z=k)
    total = VZ[z].astype(F32)
    for d in range(1, NZ):
        k = lax.rem(z + d, NZ)
        arrived(RZ.at[k], rzs.at[d], rzr.at[k], c=1 - c)
        total = total + RZ[k].astype(F32)
    dweight[...] = total
    for copy in pending:
        copy.wait_send()


def hand_over(a, b, c, a_out, b_out, c_out, sem):
    copies = [pltpu.make_async_copy(s, d, sem.at[k]) for k, (s, d) in enumerate(((a, a_out), (b, b_out), (c, c_out)))]
    for copy in copies:
        copy.start()
    for copy in copies:
        copy.wait()


def per_device(dims, tokens, proj_weight, gate_weight, conv_weight, recur_weight, input_weight, decay_param, out_grad):
    NZ, NY, NX, rows = dims
    R = rows + 2 * HALO
    share = LANES // NY
    vmem = pltpu.VMEM
    dma = pltpu.SemaphoreType.DMA
    flat = [vmem((R, LANES), F32)] * 11
    far, anywhere, inside = (pl.BlockSpec(memory_space=m) for m in (pltpu.HBM, pl.ANY, pltpu.VMEM))
    results = pl.pallas_call(
        functools.partial(kernel, dims),
        out_shape=(
            jax.ShapeDtypeStruct((rows, LANES), BF16),
            jax.ShapeDtypeStruct((rows, LANES), BF16),
            jax.ShapeDtypeStruct((share, LANES), F32),
        ),
        in_specs=[far] * 8,
        out_specs=(inside, inside, inside),
        scratch_shapes=[
            vmem((4 * NX, R, LANES), BF16),
            vmem(proj_weight.shape, BF16),
            vmem(gate_weight.shape, BF16),
            vmem((R, LANES), BF16),
            vmem((2, BLOCK, BLOCK), BF16),
            vmem((2, BLOCK, BLOCK), BF16),
            vmem((R, 2 * LANES), F32),
            vmem((R + 8, LANES), F32),
            vmem((R, LANES), BF16),
            vmem((R, 2 * LANES), F32),
            *flat,
            vmem((R, 2 * LANES), BF16),
            vmem((R + 8, LANES), F32),
            vmem((NY, NZ, share, rows), BF16),
            vmem((8, LANES), F32),
            vmem((NY, 8, LANES), F32),
            vmem((8, LANES), F32),
            vmem((NZ, 8, LANES), F32),
            vmem((8, LANES), F32),
            vmem((8, LANES), F32),
            vmem((NY, NZ, share, LANES), BF16),
            vmem((NY, NZ, share, LANES), BF16),
            vmem((NZ, share, LANES), BF16),
            vmem((NZ, share, LANES), BF16),
            dma((9,)),
            dma((2,)),
            dma((2,)),
            dma((7, 2)),
            dma((7, 2)),
            dma((2,)),
            dma((14,)),
            dma((14,)),
            dma((NY,)),
            dma((NY,)),
            dma((NZ,)),
            dma((NZ,)),
            dma((7, 2)),
            dma((7, 2)),
            dma((NZ,)),
            dma((NZ,)),
            pltpu.SemaphoreType.REGULAR((5,)),
            vmem(conv_weight.shape, F32),
            vmem((decay_param.shape[0] // LANES, LANES), F32),
        ],
        compiler_params=pltpu.CompilerParams(collective_id=0, has_side_effects=True, vmem_limit_bytes=40 * 2**20),
    )(*(pltpu.with_memory_space_constraint(a, pltpu.HBM) for a in (
        tokens, proj_weight, gate_weight, conv_weight, recur_weight, input_weight,
        decay_param.reshape(-1, LANES), out_grad,
    )))
    return pl.pallas_call(
        hand_over,
        out_shape=[jax.ShapeDtypeStruct(r.shape, r.dtype) for r in results],
        in_specs=[inside] * 3,
        out_specs=[anywhere] * 3,
        scratch_shapes=[dma((3,))],
        compiler_params=pltpu.CompilerParams(vmem_limit_bytes=2**21),
    )(*results)


def solution(mesh):
    sizes = (16, 8, 4, 2)
    split = Mesh(mesh.devices.reshape(sizes), ("z", "y", "x", "c"))
    span, group = ("z", "y"), ("x", "c")
    placed = (P(span, group), P(None, group), P(None, group), P(), P(), P(), P(), P(span, group))

    def step(*args):
        return per_device((*sizes[:3], args[0].shape[0]), *args)

    return jax.shard_map(
        step,
        mesh=split,
        in_specs=placed,
        out_specs=(P(span, group), P(span, group), P(span, group)),
        check_vma=False,
    )
```

```python
import functools

import jax
import jax.numpy as jnp
from jax import lax
from jax.experimental import pallas as pl
from jax.experimental.pallas import tpu as pltpu
from jax.sharding import Mesh
from jax.sharding import PartitionSpec as P

MESH = pl.DeviceIdType.MESH
F32 = jnp.float32
BF16 = jnp.bfloat16
BLOCK = 64
HALO = 16
LANES = 128
RATE = 8.0
FLOOR = 0.0001
GELU_A = 0.7978845608028654
GELU_B = 0.044715
CHUNK = 80


def small_expm1(x):
    p = 1.0 / 5040.0
    for c in (1.0 / 720.0, 1.0 / 120.0, 1.0 / 24.0, 1.0 / 6.0, 0.5, 1.0):
        p = p * x + c
    return p * x


def small_log1p(u):
    p = -1.0 / 6.0
    for c in (1.0 / 5.0, -1.0 / 4.0, 1.0 / 3.0, -0.5, 1.0):
        p = p * u + c
    return p * u


def kernel(
    dims, tok, pw, gw, cw_far, rw, iw, dp_far, og, dproj, dgate, dweight,
    G, WP, WG, OG, RW, IW, ACC, PJ, CV, PRE, A, B, DG, RO, IO, SC, DGL, HP, PP, YN, QN, DR, DC,
    GT, SUM, RYC, SUMZ, RZC, CF, CB, WS, RY, VZ, RZ,
    lsem, hys, hyr, hxs, hxr, ogs, ags, agr, ycs, ycr, zcs, zcr, rys, ryr, rzs, rzr, met, cw, dp,
):
    NZ, NY, NX, rows = dims
    R = rows + 2 * HALO
    SEG = R // 8
    nch = R // CHUNK
    z, y, x, c = (lax.axis_index(n) for n in ("z", "y", "x", "c"))
    sp = z * NY + y
    nsp = NZ * NY
    tp = x * 2 + c
    nxt, prv = lax.rem(sp + 1, nsp), lax.rem(sp + nsp - 1, nsp)
    nz, ny = nxt // NY, lax.rem(nxt, NY)
    pz, py = prv // NY, lax.rem(prv, NY)
    left, right, opp = lax.rem(x + NX - 1, NX), lax.rem(x + 1, NX), lax.rem(x + 2, NX)

    loads = [
        pltpu.make_async_copy(tok.at[:, pl.ds(h * LANES, LANES)], G.at[2 * tp + h, pl.ds(HALO, rows)], lsem.at[h])
        for h in range(2)
    ]
    loads += [
        pltpu.make_async_copy(pw, WP, lsem.at[2]),
        pltpu.make_async_copy(gw, WG, lsem.at[3]),
        pltpu.make_async_copy(og, OG.at[pl.ds(HALO, rows)], lsem.at[4]),
        pltpu.make_async_copy(rw.at[pl.ds(2 * tp, 2)], RW, lsem.at[5]),
        pltpu.make_async_copy(iw.at[pl.ds(2 * tp, 2)], IW, lsem.at[6]),
        pltpu.make_async_copy(cw_far, cw, lsem.at[7]),
        pltpu.make_async_copy(dp_far, dp, lsem.at[8]),
    ]
    for copy in loads:
        copy.start()

    barrier = pltpu.get_barrier_semaphore()

    def greet(**where):
        pl.semaphore_signal(barrier, inc=1, device_id=where, device_id_type=MESH)

    greet(c=1 - c)
    greet(x=left)
    greet(x=right)
    greet(z=nz, y=ny)
    greet(z=pz, y=py)
    for d in (1, NY - 1):
        greet(y=lax.rem(y + d, NY))
    for d in (1, NZ - 1):
        greet(z=lax.rem(z + d, NZ))
    pl.semaphore_wait(barrier, 9)

    def tell(sem, **where):
        pl.semaphore_signal(met.at[sem], inc=1, device_id=where, device_id_type=MESH)

    def tell_y(sem, d):
        tell(sem, y=lax.rem(y + d, NY))
        tell(sem, y=lax.rem(y + NY - d, NY))

    def tell_z(sem, d):
        tell(sem, z=lax.rem(z + d, NZ))
        tell(sem, z=lax.rem(z + NZ - d, NZ))

    far_y = sorted(range(1, NY), key=lambda d: -min(d, NY - d))
    far_z = sorted(range(1, NZ), key=lambda d: -min(d, NZ - d))
    pending = []

    def send(src, dst, ssem, rsem, **where):
        copy = pltpu.make_async_remote_copy(
            src_ref=src, dst_ref=dst, send_sem=ssem, recv_sem=rsem, device_id=where, device_id_type=MESH
        )
        copy.start()
        pending.append(copy)

    def arrived(dst, ssem, rsem, **where):
        pltpu.make_async_remote_copy(
            src_ref=dst, dst_ref=dst, send_sem=ssem, recv_sem=rsem, device_id=where, device_id_type=MESH
        ).wait_recv()

    loads[0].wait()
    loads[1].wait()
    mine = 2 * tp
    main = pl.ds(HALO, rows)
    edges = (pl.ds(0, HALO), pl.ds(HALO + rows, HALO))
    send(G.at[pl.ds(mine, 2), pl.ds(rows, HALO)], G.at[pl.ds(mine, 2), edges[0]], hys.at[0], hyr.at[0], z=nz, y=ny)
    send(G.at[pl.ds(mine, 2), pl.ds(HALO, HALO)], G.at[pl.ds(mine, 2), edges[1]], hys.at[1], hyr.at[1], z=pz, y=py)

    def halo(xx, cc, k):
        return G.at[pl.ds(4 * xx + 2 * cc, 2), edges[k]]

    def pass_halo(xx, slot, k, **where):
        send(halo(xx, c, k), halo(xx, c, k), hxs.at[slot, k], hxr.at[slot, k], **where)

    def got_halo(xx, cc, slot, k):
        arrived(halo(xx, cc, k), hxs.at[slot, k], hxr.at[slot, k], c=1 - c)

    def piece(xx, cc, h):
        return 4 * xx + 2 * cc + h

    def give(i, sem, **where):
        send(G.at[i, main], G.at[i, main], ags.at[sem], agr.at[sem], **where)

    def got(i, sem):
        arrived(G.at[i, main], ags.at[sem], agr.at[sem], c=1 - c)

    p0, p1 = piece(x, c, 0), piece(x, c, 1)
    give(p0, 0, x=right)
    give(p1, 1, x=left)
    give(p0, 6, c=1 - c)
    give(p1, 7, c=1 - c)
    loads[4].wait()
    send(OG.at[pl.ds(HALO, HALO)], OG.at[pl.ds(HALO + rows, HALO)], ogs.at[0], ogs.at[1], z=pz, y=py)
    tell_y(0, 1)
    tell_z(1, 1)
    for k in (2, 3, 5, 6, 7, 8):
        loads[k].wait()

    OG[pl.ds(0, HALO), :] = jnp.zeros((HALO, LANES), BF16)
    PJ[pl.ds(0, 8), :] = jnp.zeros((8, LANES), F32)
    DC[pl.ds(R, 8), :] = jnp.zeros((8, LANES), F32)
    slope = -RATE * small_log1p(jnp.exp(-dp[pl.ds(tp, 1), :]))
    taps = [cw[pl.ds(k, 1), pl.ds(pl.multiple_of(tp * LANES, LANES), LANES)] for k in range(4)]
    zero = jnp.zeros((BLOCK, BLOCK), BF16)
    gates = jnp.concatenate(
        [
            jnp.concatenate([RW[0], zero, IW[0], zero], axis=1),
            jnp.concatenate([zero, RW[1], zero, IW[1]], axis=1),
        ],
        axis=0,
    )

    for k in range(2):
        arrived(halo(x, c, k), hys.at[k], hyr.at[k], c=1 - c)
        pass_halo(x, 0, k, x=right)
        pass_halo(x, 1, k, x=left)
        pass_halo(x, 3, k, c=1 - c)
    give(p1, 2, x=right)
    give(p0, 3, x=left)
    arrived(OG.at[pl.ds(HALO + rows, HALO)], ogs.at[0], ogs.at[1], c=1 - c)

    @pl.when(sp == nsp - 1)
    def _():
        OG[pl.ds(HALO + rows, HALO), :] = jnp.zeros((HALO, LANES), BF16)

    def multiply(i0, i1, first=False):
        def half(i):
            at = pl.ds(pl.multiple_of(i * LANES, LANES), LANES)
            return jnp.concatenate([WP[at, :], WG[at, :]], axis=1)

        rhs = jnp.concatenate([half(i0), half(i1)], axis=0)
        lhs = jnp.concatenate([G[i0], G[i1]], axis=1)
        out = jnp.dot(lhs, rhs, preferred_element_type=F32)
        if first:
            ACC[...] = out
        else:
            ACC[...] += out

    pl.semaphore_wait(met.at[0], 2)
    pl.semaphore_wait(met.at[1], 2)
    tell_y(2, 2)
    tell_z(3, 2)
    multiply(p0, p1, True)
    got(piece(x, 1 - c, 0), 6)
    got(piece(x, 1 - c, 1), 7)
    for k in range(2):
        got_halo(x, 1 - c, 3, k)
    multiply(piece(x, 1 - c, 0), piece(x, 1 - c, 1))

    l0, l1 = piece(left, c, 0), piece(left, c, 1)
    r0, r1 = piece(right, c, 0), piece(right, c, 1)
    o0, o1 = piece(opp, c, 0), piece(opp, c, 1)
    got(l0, 0)
    for k in range(2):
        got_halo(left, c, 0, k)
    pass_halo(left, 2, 0, x=right)
    give(l0, 4, x=right)
    give(l0, 8, c=1 - c)
    got(r1, 1)
    for k in range(2):
        got_halo(right, c, 1, k)
    pass_halo(right, 2, 1, x=left)
    give(r1, 5, x=left)
    give(r1, 9, c=1 - c)
    for k in range(2):
        pass_halo(left, 4, k, c=1 - c)
        pass_halo(right, 5, k, c=1 - c)
    multiply(l0, r1)
    got(piece(left, 1 - c, 0), 8)
    got(piece(right, 1 - c, 1), 9)
    for k in range(2):
        got_halo(left, 1 - c, 4, k)
        got_halo(right, 1 - c, 5, k)
    multiply(piece(left, 1 - c, 0), piece(right, 1 - c, 1))
    pl.semaphore_wait(met.at[2], 2)
    pl.semaphore_wait(met.at[3], 2)
    tell_z(4, 4)
    got(l1, 2)
    give(l1, 10, c=1 - c)
    got(r0, 3)
    give(r0, 11, c=1 - c)
    multiply(l1, r0)
    got(piece(left, 1 - c, 1), 10)
    got(piece(right, 1 - c, 0), 11)
    multiply(piece(left, 1 - c, 1), piece(right, 1 - c, 0))
    pl.semaphore_wait(met.at[4], 2)
    for k in range(2):
        got_halo(opp, c, 2, k)
        pass_halo(opp, 6, k, c=1 - c)
    got(o0, 4)
    give(o0, 12, c=1 - c)
    got(o1, 5)
    give(o1, 13, c=1 - c)
    multiply(o0, o1)
    got(piece(opp, 1 - c, 0), 12)
    got(piece(opp, 1 - c, 1), 13)
    for k in range(2):
        got_halo(opp, 1 - c, 6, k)
    multiply(piece(opp, 1 - c, 0), piece(opp, 1 - c, 1))

    PJ[pl.ds(8, R), :] = ACC[:, pl.ds(0, LANES)].astype(BF16).astype(F32)

    @pl.when(sp == 0)
    def _():
        PJ[pl.ds(8, HALO), :] = jnp.zeros((HALO, LANES), F32)

    def convolve(i, _):
        base = pl.multiple_of(i * CHUNK, CHUNK)
        part = PJ[pl.ds(base, CHUNK + 8), :]
        total = taps[0] * part[8:]
        for k in range(1, 4):
            total = total + taps[k] * pltpu.roll(part, k, 0)[8:]
        CV[pl.ds(base, CHUNK), :] = total.astype(BF16)
        return 0

    lax.fori_loop(0, nch, convolve, 0)
    PRE[...] = jnp.dot(CV[...], gates, preferred_element_type=F32)

    def local(i, _):
        base = pl.multiple_of(i * CHUNK, CHUNK)
        at = pl.ds(base, CHUNK)
        ro = jax.nn.sigmoid(PRE[at, pl.ds(0, LANES)])
        io = jax.nn.sigmoid(PRE[at, pl.ds(LANES, LANES)])
        conv = CV[at, :].astype(F32)
        e = small_expm1(slope * ro)
        sc = jnp.sqrt(FLOOR - e * (2.0 + e))
        row = lax.broadcasted_iota(jnp.int32, (CHUNK, LANES), 0) + base
        own = row >= HALO
        A[at, :] = jnp.where(own, 1.0 + e, 1.0)
        B[at, :] = jnp.where(own, sc * (io * conv), 0.0)
        RO[at, :] = ro
        IO[at, :] = io
        SC[at, :] = sc
        q = ACC[at, pl.ds(LANES, LANES)].astype(BF16).astype(F32)
        cot = OG[at, :].astype(F32)
        t = jnp.tanh(GELU_A * (q + GELU_B * (q * q * q)))
        cdf = 0.5 * (1.0 + t)
        DG[at, :] = cot * (q * cdf)
        DGL[at, :] = t
        return 0

    lax.fori_loop(0, nch, local, 0)

    STEP = 10

    def scan(i, carry):
        h, p, yb, q = carry
        for k in range(STEP):
            v = i * STEP + k
            fw, bw = pl.ds(v, 8, stride=SEG), pl.ds(SEG - 1 - v, 8, stride=SEG)
            a, b = A[fw, :], B[fw, :]
            HP[fw, :] = h
            PP[fw, :] = p
            h = a * h + b
            p = p * a
            a, g = A[bw, :], DG[bw, :]
            YN[bw, :] = yb
            QN[bw, :] = q
            yb = a * (g + yb)
            q = q * a
        return h, p, yb, q

    one, nil = jnp.ones((8, LANES), F32), jnp.zeros((8, LANES), F32)
    h, p, yb, q = lax.fori_loop(0, SEG // STEP, scan, (nil, one, nil, one))

    fa, fs, s_of, a_of = one[0:1], nil[0:1], [], []
    for k in range(8):
        s_of.append(fs)
        a_of.append(fa)
        fs = h[k : k + 1] + p[k : k + 1] * fs
        fa = fa * p[k : k + 1]
    ba, bs, t_of, c_of = one[0:1], nil[0:1], [None] * 8, [None] * 8
    for k in reversed(range(8)):
        t_of[k] = bs
        c_of[k] = ba
        bs = yb[k : k + 1] + q[k : k + 1] * bs
        ba = ba * q[k : k + 1]
    last, lead = HALO + rows - 1, 2 * HALO
    ls, fsg = last // SEG, lead // SEG
    la, lb = A[pl.ds(last, 1), :], B[pl.ds(last, 1), :]
    lp = PP[pl.ds(last, 1), :]
    out_a = la * lp * a_of[ls]
    out_s = la * (HP[pl.ds(last, 1), :] + lp * s_of[ls]) + lb
    ga, gg = A[pl.ds(lead, 1), :], DG[pl.ds(lead, 1), :]
    gq = QN[pl.ds(lead, 1), :]
    out_c = ga * gq * c_of[fsg]
    out_l = ga * (gg + YN[pl.ds(lead, 1), :] + gq * t_of[fsg])

    def put(ref, values):
        for k, value in enumerate(values):
            ref[pl.ds(k, 1), :] = value

    share = LANES // NY
    SUM[...] = nil
    put(SUM, (out_a, out_s, out_c, out_l))
    for d in far_y:
        send(SUM, RYC.at[y], ycs.at[d], ycr.at[y], y=lax.rem(y + d, NY))
    RYC[y] = SUM[...]

    def factors(i, _):
        at = pl.ds(pl.multiple_of(i * CHUNK, CHUNK), CHUNK)
        a, ro, io, sc = A[at, :], RO[at, :], IO[at, :], SC[at, :]
        conv = CV[at, :].astype(F32)
        q = ACC[at, pl.ds(LANES, LANES)].astype(BF16).astype(F32)
        t = DGL[at, :]
        slant = 0.5 * (1.0 + t) + 0.5 * q * (1.0 - t * t) * (GELU_A * (1.0 + 3.0 * GELU_B * (q * q)))
        DGL[at, :] = OG[at, :].astype(F32) * slant
        both = sc * io
        PRE[at, pl.ds(0, LANES)] = (io * conv) * a * a / sc
        RO[at, :] = slope * ro * (1.0 - ro)
        IO[at, :] = both
        SC[at, :] = both * conv * (1.0 - io)
        return 0

    lax.fori_loop(0, nch, factors, 0)

    def turn(i, _):
        GT[:, i] = G[i, main, :].T.reshape(NY, share, rows)
        return 0

    lax.fori_loop(0, NZ // 2, turn, 0)
    for d in range(1, NY):
        k = lax.rem(y + d, NY)
        arrived(RYC.at[k], ycs.at[d], ycr.at[k], c=1 - c)

    def compose(ref, count, place):
        fa, fs, fai, fsi = one[0:1], nil[0:1], one[0:1], nil[0:1]
        for k in range(count):
            a, s = ref[k, pl.ds(0, 1), :], ref[k, pl.ds(1, 1), :]
            fa, fs = fa * a, a * fs + s
            before = k < place
            fai, fsi = jnp.where(before, fa, fai), jnp.where(before, fs, fsi)
        ba, bs, bai, bsi = one[0:1], nil[0:1], one[0:1], nil[0:1]
        for k in reversed(range(count)):
            a, s = ref[k, pl.ds(2, 1), :], ref[k, pl.ds(3, 1), :]
            ba, bs = ba * a, a * bs + s
            after = k > place
            bai, bsi = jnp.where(after, ba, bai), jnp.where(after, bs, bsi)
        return (fa, fs, ba, bs), (fai, fsi, bai, bsi)

    total, inside = compose(RYC, NY, y)
    SUMZ[...] = nil
    put(SUMZ, total)
    for d in far_z:
        send(SUMZ, RZC.at[z], zcs.at[d], zcr.at[z], z=lax.rem(z + d, NZ))
    RZC[z] = SUMZ[...]
    lax.fori_loop(NZ // 2, NZ, turn, 0)
    for d in range(1, NZ):
        k = lax.rem(z + d, NZ)
        arrived(RZC.at[k], zcs.at[d], zcr.at[k], c=1 - c)
    _, outer = compose(RZC, NZ, z)
    carry_s = inside[1] + inside[0] * outer[1]
    carry_g = inside[3] + inside[2] * outer[3]
    put(CF, [s_of[k] + a_of[k] * carry_s for k in range(8)])
    put(CB, [t_of[k] + c_of[k] * carry_g for k in range(8)])
    cf, cb = CF[...], CB[...]

    def finish(i, _):
        for k in range(STEP):
            at = pl.ds(i * STEP + k, 8, stride=SEG)
            HP[at, :] = HP[at, :] + PP[at, :] * cf
            YN[at, :] = YN[at, :] + QN[at, :] * cb
        return 0

    lax.fori_loop(0, SEG // STEP, finish, 0)

    def gradients(i, _):
        base = pl.multiple_of(i * CHUNK, CHUNK)
        at = pl.ds(base, CHUNK)
        grad = DG[at, :] + YN[at, :]
        d_log = grad * (A[at, :] * HP[at, :] - PRE[at, pl.ds(0, LANES)])
        DR[at, pl.ds(0, LANES)] = (d_log * RO[at, :]).astype(BF16)
        DR[at, pl.ds(LANES, LANES)] = (grad * SC[at, :]).astype(BF16)
        DC[at, :] = grad * IO[at, :]
        return 0

    lax.fori_loop(0, nch, gradients, 0)
    DC[pl.ds(0, R), :] += lax.dot_general(DR[...], gates, (((1,), (1,)), ((), ())), preferred_element_type=F32)

    WIDE = 96

    def unconvolve(i, _):
        base = pl.multiple_of(i * WIDE, WIDE)
        part = DC[pl.ds(base + HALO, WIDE + 8), :]
        total = taps[0] * part[:WIDE]
        for k in range(1, 4):
            total = total + taps[k] * pltpu.roll(part, WIDE + 8 - k, 0)[:WIDE]
        dproj[pl.ds(base, WIDE), :] = total.astype(BF16)
        return 0

    lax.fori_loop(0, rows // WIDE, unconvolve, 0)

    grad = dproj[...]
    half = NZ // 2
    sides = [pl.ds(0, half), pl.ds(half, half)]

    def along(d):
        return lax.rem(y + NY + d, NY)

    def partial(d):
        k = along(d)
        part = jnp.dot(GT[k].reshape(NZ * share, rows), grad, preferred_element_type=F32)
        WS[k] = part.astype(BF16).reshape(NZ, share, LANES)
        return k

    def hop(k, h, slot, d):
        send(WS.at[k, sides[h]], RY.at[slot, sides[h]], rys.at[slot, h], ryr.at[slot, h], y=along(d))

    def landed(slot, h):
        arrived(RY.at[slot, sides[h]], rys.at[slot, h], ryr.at[slot, h], c=1 - c)

    def add(k, h, slot):
        landed(slot, h)
        WS[k, sides[h]] = (WS[k, sides[h]].astype(F32) + RY[slot, sides[h]].astype(F32)).astype(BF16)

    k = partial(4)
    hop(k, 0, 0, 2)
    hop(k, 1, 0, -2)
    k = partial(3)
    hop(k, 0, 1, 2)
    hop(k, 1, 1, 2)
    k = partial(-3)
    hop(k, 0, 2, -2)
    hop(k, 1, 2, -2)
    hop(partial(2), 1, 3, 2)
    hop(partial(-2), 0, 4, -2)
    partial(1)
    partial(-1)
    partial(0)
    dgate[...] = (DGL[pl.ds(HALO, rows), :] * (A[pl.ds(HALO, rows), :] * HP[pl.ds(HALO, rows), :] + B[pl.ds(HALO, rows), :])).astype(BF16)
    add(along(2), 0, 0)
    hop(along(2), 0, 3, 2)
    add(along(-2), 1, 0)
    hop(along(-2), 1, 4, -2)
    for h in range(2):
        add(along(1), h, 1)
        hop(along(1), h, 5, 1)
        add(along(-1), h, 2)
        hop(along(-1), h, 6, -1)
    for h in range(2):
        total = WS[y, sides[h]].astype(F32)
        for slot in (3, 4, 5, 6):
            landed(slot, h)
            total = total + RY[slot, sides[h]].astype(F32)
        VZ[sides[h]] = total.astype(BF16)
    for d in far_z:
        k = lax.rem(z + d, NZ)
        send(VZ.at[k], RZ.at[z], rzs.at[d], rzr.at[z], z=k)
    total = VZ[z].astype(F32)
    for d in range(1, NZ):
        k = lax.rem(z + d, NZ)
        arrived(RZ.at[k], rzs.at[d], rzr.at[k], c=1 - c)
        total = total + RZ[k].astype(F32)
    dweight[...] = total
    for copy in pending:
        copy.wait_send()


def hand_over(a, b, c, a_out, b_out, c_out, sem):
    copies = [pltpu.make_async_copy(s, d, sem.at[k]) for k, (s, d) in enumerate(((a, a_out), (b, b_out), (c, c_out)))]
    for copy in copies:
        copy.start()
    for copy in copies:
        copy.wait()


def per_device(dims, tokens, proj_weight, gate_weight, conv_weight, recur_weight, input_weight, decay_param, out_grad):
    NZ, NY, NX, rows = dims
    R = rows + 2 * HALO
    share = LANES // NY
    vmem = pltpu.VMEM
    dma = pltpu.SemaphoreType.DMA
    flat = [vmem((R, LANES), F32)] * 11
    far, anywhere, inside = (pl.BlockSpec(memory_space=m) for m in (pltpu.HBM, pl.ANY, pltpu.VMEM))
    results = pl.pallas_call(
        functools.partial(kernel, dims),
        out_shape=(
            jax.ShapeDtypeStruct((rows, LANES), BF16),
            jax.ShapeDtypeStruct((rows, LANES), BF16),
            jax.ShapeDtypeStruct((share, LANES), F32),
        ),
        in_specs=[far] * 8,
        out_specs=(inside, inside, inside),
        scratch_shapes=[
            vmem((4 * NX, R, LANES), BF16),
            vmem(proj_weight.shape, BF16),
            vmem(gate_weight.shape, BF16),
            vmem((R, LANES), BF16),
            vmem((2, BLOCK, BLOCK), BF16),
            vmem((2, BLOCK, BLOCK), BF16),
            vmem((R, 2 * LANES), F32),
            vmem((R + 8, LANES), F32),
            vmem((R, LANES), BF16),
            vmem((R, 2 * LANES), F32),
            *flat,
            vmem((R, 2 * LANES), BF16),
            vmem((R + 8, LANES), F32),
            vmem((NY, NZ, share, rows), BF16),
            vmem((8, LANES), F32),
            vmem((NY, 8, LANES), F32),
            vmem((8, LANES), F32),
            vmem((NZ, 8, LANES), F32),
            vmem((8, LANES), F32),
            vmem((8, LANES), F32),
            vmem((NY, NZ, share, LANES), BF16),
            vmem((NY, NZ, share, LANES), BF16),
            vmem((NZ, share, LANES), BF16),
            vmem((NZ, share, LANES), BF16),
            dma((9,)),
            dma((2,)),
            dma((2,)),
            dma((7, 2)),
            dma((7, 2)),
            dma((2,)),
            dma((14,)),
            dma((14,)),
            dma((NY,)),
            dma((NY,)),
            dma((NZ,)),
            dma((NZ,)),
            dma((7, 2)),
            dma((7, 2)),
            dma((NZ,)),
            dma((NZ,)),
            pltpu.SemaphoreType.REGULAR((5,)),
            vmem(conv_weight.shape, F32),
            vmem((decay_param.shape[0] // LANES, LANES), F32),
        ],
        compiler_params=pltpu.CompilerParams(collective_id=0, has_side_effects=True, vmem_limit_bytes=40 * 2**20),
    )(*(pltpu.with_memory_space_constraint(a, pltpu.HBM) for a in (
        tokens, proj_weight, gate_weight, conv_weight, recur_weight, input_weight,
        decay_param.reshape(-1, LANES), out_grad,
    )))
    return pl.pallas_call(
        hand_over,
        out_shape=[jax.ShapeDtypeStruct(r.shape, r.dtype) for r in results],
        in_specs=[inside] * 3,
        out_specs=[anywhere] * 3,
        scratch_shapes=[dma((3,))],
        compiler_params=pltpu.CompilerParams(vmem_limit_bytes=2**21),
    )(*results)


def solution(mesh):
    sizes = (16, 8, 4, 2)
    split = Mesh(mesh.devices.reshape(sizes), ("z", "y", "x", "c"))
    span, group = ("z", "y"), ("x", "c")
    placed = (P(span, group), P(None, group), P(None, group), P(), P(), P(), P(), P(span, group))

    def step(*args):
        return per_device((*sizes[:3], args[0].shape[0]), *args)

    return jax.shard_map(
        step,
        mesh=split,
        in_specs=placed,
        out_specs=(P(span, group), P(span, group), P(span, group)),
        check_vma=False,
    )
```
